128 devices in a mesh: sp: 16 (over z, y), dp: 8 (over x, core).
Axes of the slice: x: 4, y: 4, z: 4, core: 2. Of those that a mesh axis runs over, the one named last changes fastest.
Arguments:
- stream: bfloat16 [8, 2048, 2048], P('dp', 'sp'), may hold values from -6 to 6
- query_proj: bfloat16 [8, 2048, 2048], P('dp', 'sp'), may hold values from -6 to 6
- key_proj: bfloat16 [8, 2048, 2048], P('dp', 'sp'), may hold values from -6 to 6
- value_proj: bfloat16 [8, 2048, 2048], P('dp', 'sp'), may hold values from -6 to 6
- out_gate: bfloat16 [8, 2048, 2048], P('dp', 'sp'), may hold values from -6 to 6
- beta_logit: bfloat16 [8, 2048, 16], P('dp', 'sp'), may hold values from -6 to 6
- log_decay: float32 [8, 16, 2048], P('dp', 'sp'), may hold values from -0.8 to 0, as said below
- head_gain: float32 [128], replicated, may hold values from 0.1 to 1.9
- out_proj: bfloat16 [2048, 2048], replicated, may hold values from -0.125 to 0.125
- ffn_gain: float32 [2048], replicated, may hold values from 0.1 to 1.9
- routes: int32 [8, 2048, 2], P('dp', 'sp'), may hold values from 0 to 15, all different within a row; in each aligned block of 128 rows (0 to 127, 128 to 255, ..., all dimensions but the last counted through in order) at most 32 rows name the same one
- route_weight: float32 [8, 2048, 2], P('dp', 'sp'), may hold values from 0.1 to 1
- expert_gate: bfloat16 [16, 2048, 5120], P('sp', None, 'dp'), may hold values from -0.125 to 0.125
- expert_up: bfloat16 [16, 2048, 5120], P('sp', None, 'dp'), may hold values from -0.125 to 0.125
- expert_down: bfloat16 [16, 5120, 2048], P('sp', 'dp'), may hold values from -0.078125 to 0.078125
Outputs:
- result: bfloat16 [8, 2048, 2048], P('dp', 'sp')
The draws below stay inside these ranges and needn't reach their ends.
Inputs may be any that keep to these rules, and one draw needn't show every extreme that they name: `routes`: each row names 2 different experts; within the rows of one device no expert is named more than 32 times, and some devices reach 32. log_decay is never positive.
All inputs are finite; a program needn't handle non-finite values.
Results may differ from the reference program's by a relative error of at most 0.0085.
Values may be sent and summed in bfloat16 or wider, within the bound.
No kernel may reach another device: no remote copies, remote signals or barrier semaphores. Data moves between devices by JAX's collectives and lax.ppermute only.
A program may use at most 128 MiB of HBM per device.

```python
import math
import jax
import jax.numpy as jnp
import numpy as np
from jax import lax

D = 2048
MIXER_HEADS = 16
HEAD_DIM = 128
FF = 5120
TOP = 2
BLOCK_LEN = 64
TOK_DEV = 128
SEQUENCE_COUNT = 8
SEQUENCE_LENGTH = 2048
EXPERTS = 16
CAP = 32
N_SP = 16
N_DP = 8


def draw_log_decay(key, part):
    random_split_keys = jax.random.split(jax.random.fold_in(key, 11), 5)
    quick_heads = jax.random.uniform(random_split_keys[0], (1, MIXER_HEADS, 1)) < 0.5
    n_blocks = SEQUENCE_LENGTH // TOK_DEV
    scale_per_block = jnp.exp(jax.random.uniform(random_split_keys[1], (SEQUENCE_COUNT, 1, n_blocks), minval=-0.7, maxval=0.7))
    scale_per_block = jnp.repeat(scale_per_block, TOK_DEV, axis=2)
    random_noise = jax.random.uniform(random_split_keys[2], (SEQUENCE_COUNT, MIXER_HEADS, SEQUENCE_LENGTH), minval=0.25, maxval=1.75)
    baseline_rate = jnp.where(quick_heads, 1.0 / 40.0, 0.5 / SEQUENCE_LENGTH)
    spike_position = jax.random.randint(random_split_keys[3], (SEQUENCE_COUNT, 1, 2), 0, SEQUENCE_LENGTH)
    token_position = jnp.arange(SEQUENCE_LENGTH)[None, None, :, None]
    spike_selected = jnp.any(token_position == spike_position[:, :, None, :], axis=-1)
    spike_magnitude = jax.random.uniform(random_split_keys[4], (SEQUENCE_COUNT, MIXER_HEADS, SEQUENCE_LENGTH), minval=0.22, maxval=0.69)
    return -(baseline_rate * scale_per_block * random_noise) - jnp.where(spike_selected, spike_magnitude, 0.0)


def level_of(rng, dims, cuts, least, largest):
    level = 1.0
    for dim, shards_of in cuts:
        steps = jax.random.uniform(jax.random.fold_in(jax.random.fold_in(rng, 6), dim), (shards_of,), jnp.float32, least / len(cuts), largest / len(cuts))
        level = level * jnp.repeat(jnp.exp(steps), dims[dim] // shards_of).reshape((-1,) + (1,) * (len(dims) - 1 - dim))
    return level


def assign_block(stream_key, own, number, rows, count, top, limit, slope):
    order = jax.random.permutation(stream_key, count)
    heavy_load, usual = portions_of(count, rows * top, limit, slope, True), portions_of(count, rows * top, limit, slope, False)
    places = jnp.arange(count)

    def named(tallies, rotation):
        used = int((tallies > 0).sum())
        fixed = max(1, used // 4)
        shifted = fixed + (places - fixed + rotation * (used - fixed)) % max(1, count - fixed)
        return jnp.zeros((count,), jnp.int32).at[order[jnp.where(places < fixed, places, shifted)]].set(jnp.asarray(tallies, jnp.int32))

    tallies = jnp.where(number % 4 == 0, named(heavy_load, number // 4), named(usual, number - number // 4 - 1))
    mixed = jax.random.permutation(jax.random.fold_in(own, 3), count)
    giver, receiver = mixed[0:count // 2 * 2:2], mixed[1:count // 2 * 2:2]
    room = jnp.minimum(tallies[giver] - 1, limit - tallies[receiver]) // 2
    room = jnp.where((giver == order[0]) | (receiver == order[0]) | (tallies[receiver] == 0), 0, jnp.maximum(room, 0))
    shifted = jax.random.randint(jax.random.fold_in(own, 4), (count // 2,), 0, 1 << 20) % (room + 1)
    tallies = tallies.at[giver].add(-shifted).at[receiver].add(shifted)
    items = jnp.searchsorted(jnp.cumsum(tallies), jnp.arange(rows * top), side="right").astype(jnp.int32)
    grid = items.reshape(top, rows).T
    grid = grid[jax.random.permutation(jax.random.fold_in(own, 1), rows)]
    rotation = jax.random.randint(jax.random.fold_in(own, 2), (rows, 1), 0, top)
    return jnp.take_along_axis(grid, (jnp.arange(top)[None, :] + rotation) % top, axis=1)


def portions_of(amount, total, limit, lean, full):
    weights = [(1 << 20) // math.isqrt(standing ** lean) + 1 for standing in range(1, amount + 1)]
    largest = limit if full else min(limit, max(-(-total // amount), total * weights[0] // sum(weights)))
    least = 1 if total - largest >= amount - 1 else 0
    holding, spare = [largest] + [least] * (amount - 1), total - largest - least * (amount - 1)
    while spare > 0:
        free = [i for i in range(1, amount) if holding[i] < largest] or [i for i in range(1, amount) if holding[i] < limit]
        mass, budget = sum([weights[i] for i in free]), spare
        for i in free:
            more = min(limit - holding[i], max(1, budget * weights[i] // mass), spare)
            holding[i] = holding[i] + more
            spare = spare - more
    return np.array(holding)


def bell_draw(rng, shape, width, most, shards=(), kind=jnp.bfloat16):
    values = jax.random.normal(rng, shape, jnp.float32) * width
    if len(shards) > 0:
        values = level_of(rng, shape, shards, -0.22, 0.18) * values
    return jnp.clip(values, min=-most, max=most).astype(kind)


def setup_inputs(seed: int = 0) -> dict:
    key_of = jax.random.split(jax.random.key(seed), 16)
    stream = bell_draw(key_of[0], (SEQUENCE_COUNT, SEQUENCE_LENGTH, D), 1.0, 6.0, ((0, 8), (1, 16)))
    query_proj = bell_draw(key_of[1], (SEQUENCE_COUNT, SEQUENCE_LENGTH, MIXER_HEADS * HEAD_DIM), 1.0, 6.0, ((0, 8), (1, 16)))
    key_proj = bell_draw(key_of[2], (SEQUENCE_COUNT, SEQUENCE_LENGTH, MIXER_HEADS * HEAD_DIM), 1.0, 6.0, ((0, 8), (1, 16)))
    value_proj = bell_draw(key_of[3], (SEQUENCE_COUNT, SEQUENCE_LENGTH, MIXER_HEADS * HEAD_DIM), 1.0, 6.0, ((0, 8), (1, 16)))
    out_gate = bell_draw(key_of[4], (SEQUENCE_COUNT, SEQUENCE_LENGTH, MIXER_HEADS * HEAD_DIM), 1.0, 6.0, ((0, 8), (1, 16)))
    beta_logit = bell_draw(key_of[5], (SEQUENCE_COUNT, SEQUENCE_LENGTH, MIXER_HEADS), 1.5, 6.0, ((0, 8), (1, 16)))
    log_decay = draw_log_decay(jax.random.fold_in(key_of[15], 71), 0)
    head_gain = jnp.clip(1.0 + 0.18 * jax.random.normal(key_of[7], (HEAD_DIM,), jnp.float32), 0.1, 1.9)
    out_proj = bell_draw(key_of[8], (MIXER_HEADS * HEAD_DIM, D), (MIXER_HEADS * HEAD_DIM) ** -0.5, 0.125)
    ffn_gain = jnp.clip(1.0 + 0.18 * jax.random.normal(key_of[9], (D,), jnp.float32), 0.1, 1.9)
    routes_keys = jax.random.split(jax.random.fold_in(key_of[10], 1), SEQUENCE_COUNT * SEQUENCE_LENGTH // TOK_DEV)
    routes_turns = jax.random.permutation(jax.random.fold_in(key_of[10], 3), SEQUENCE_COUNT * SEQUENCE_LENGTH // TOK_DEV)
    routes = jax.vmap(lambda own, number: assign_block(jax.random.fold_in(key_of[10], 2), own, number, TOK_DEV, EXPERTS, TOP, CAP, 2))(routes_keys, routes_turns).reshape((SEQUENCE_COUNT, SEQUENCE_LENGTH, TOP))
    route_weight = jnp.clip(0.1 + 0.9 * jax.random.uniform(key_of[11], (SEQUENCE_COUNT, SEQUENCE_LENGTH, TOP), jnp.float32) ** level_of(key_of[11], (SEQUENCE_COUNT, SEQUENCE_LENGTH, TOP), ((0, 8), (1, 16)), -0.2, 0.2), 0.1, 1.0)
    expert_gate = bell_draw(key_of[12], (EXPERTS, D, FF), D ** -0.5, 0.125, ((0, 16), (2, 8)))
    expert_up = bell_draw(key_of[13], (EXPERTS, D, FF), D ** -0.5, 0.125, ((0, 16), (2, 8)))
    expert_down = bell_draw(key_of[14], (EXPERTS, FF, D), FF ** -0.5, 0.078125, ((0, 16), (1, 8)))
    return dict(stream=stream, query_proj=query_proj, key_proj=key_proj, value_proj=value_proj, out_gate=out_gate, beta_logit=beta_logit, log_decay=log_decay, head_gain=head_gain, out_proj=out_proj, ffn_gain=ffn_gain, routes=routes, route_weight=route_weight, expert_gate=expert_gate, expert_up=expert_up, expert_down=expert_down)


EPSILON = 1e-06
TOP_PRECISION = lax.Precision.HIGHEST

def unit_rows(matrix):
    return matrix * lax.rsqrt(lax.optimization_barrier(jnp.sum(matrix * matrix, axis=-1, keepdims=True)) + EPSILON)

def delta_blocks(queries, key_rows, values_in, log_rate, strength):
    length, n_heads, key_dim = key_rows.shape
    n_blocks = length // BLOCK_LEN

    def blocked(tensor):
        return tensor.reshape(n_blocks, BLOCK_LEN, n_heads, -1).transpose(0, 2, 1, 3)
    query_blk, key_blk, value_blk = (blocked(queries), blocked(key_rows), blocked(values_in))
    cumulative = jnp.cumsum(log_rate.reshape(n_blocks, BLOCK_LEN, n_heads).transpose(0, 2, 1), axis=-1)
    beta_blk = strength.reshape(n_blocks, BLOCK_LEN, n_heads).transpose(0, 2, 1)
    rows_idx = lax.broadcasted_iota(jnp.int32, (BLOCK_LEN, BLOCK_LEN), 0)
    cols_idx = lax.broadcasted_iota(jnp.int32, (BLOCK_LEN, BLOCK_LEN), 1)
    below_incl = rows_idx >= cols_idx
    strict = rows_idx > cols_idx
    decay_mat = jnp.exp(jnp.where(below_incl, cumulative[..., :, None] - cumulative[..., None, :], -jnp.inf))
    key_beta = key_blk * beta_blk[..., None]
    lower_mat = jnp.where(strict, jnp.einsum('nhid,nhjd->nhij', key_beta, key_blk, precision=TOP_PRECISION) * decay_mat, 0.0)
    system = jnp.eye(BLOCK_LEN, dtype=jnp.float32) + lower_mat
    rhs_cols = jnp.concatenate([value_blk * beta_blk[..., None], key_beta * jnp.exp(cumulative)[..., None]], axis=-1)
    solved = jax.scipy.linalg.solve_triangular(system, rhs_cols, lower=True, unit_diagonal=True)
    value_dim = value_blk.shape[-1]
    update, weight = (solved[..., :value_dim], solved[..., value_dim:])
    inside = jnp.einsum('nhid,nhjd->nhij', query_blk, key_blk, precision=TOP_PRECISION) * decay_mat

    def advance(running_state, inputs):
        query_inner, key_i, update_inner, weight_inner, running_total_inner, inside_i = inputs
        incoming_values = update_inner - jnp.einsum('nli,nif->nlf', weight_inner, running_state, precision=TOP_PRECISION)
        result = jnp.einsum('nli,nif->nlf', query_inner * jnp.exp(running_total_inner)[..., None], running_state, precision=TOP_PRECISION)
        result = result + jnp.einsum('hij,hjv->hiv', inside_i, incoming_values, precision=TOP_PRECISION)
        final_running_total = running_total_inner[:, -1:]
        trailing_key = key_i * jnp.exp(final_running_total - running_total_inner)[..., None]
        running_state = running_state * jnp.exp(final_running_total)[..., None] + jnp.einsum('gbj,gbs->gjs', trailing_key, incoming_values, precision=TOP_PRECISION)
        return (running_state, result)
    zero_state = jnp.zeros((n_heads, key_dim, value_dim), jnp.float32)
    _, results = lax.scan(advance, zero_state, (query_blk, key_blk, update, weight, cumulative, inside))
    return results.transpose(0, 2, 1, 3).reshape(length, n_heads, value_dim)

def mix_sequence(query_in, key_in, value_in, beta_in, decay_in):
    length = query_in.shape[0]
    n_heads = beta_in.shape[1]
    queries = unit_rows(query_in.reshape(length, n_heads, HEAD_DIM).astype(jnp.float32)) * HEAD_DIM ** (-0.5)
    key_rows = unit_rows(key_in.reshape(length, n_heads, HEAD_DIM).astype(jnp.float32))
    values_in = value_in.reshape(length, n_heads, HEAD_DIM).astype(jnp.float32)
    strength = jax.nn.sigmoid(beta_in.astype(jnp.float32))
    log_rate = decay_in.astype(jnp.float32).T

    def two_ways(tensor):
        return jnp.concatenate([tensor, tensor[::-1]], axis=1)
    reads = delta_blocks(two_ways(queries), two_ways(key_rows), two_ways(values_in), two_ways(log_rate), two_ways(strength))
    summed = reads[:, :n_heads] + reads[::-1, n_heads:]
    return summed.astype(jnp.bfloat16).reshape(length, n_heads * HEAD_DIM)

def reference(stream, query_proj, key_proj, value_proj, out_gate, beta_logit, log_decay, head_gain, out_proj, ffn_gain, routes, route_weight, expert_gate, expert_up, expert_down):

    def one_sequence(inputs):
        return mix_sequence(*inputs)
    mixed = lax.map(one_sequence, (query_proj, key_proj, value_proj, beta_logit, log_decay))
    model_width = stream.shape[2]
    n_tokens = stream.shape[0] * stream.shape[1]
    per_head = mixed.reshape(n_tokens, MIXER_HEADS, HEAD_DIM).astype(jnp.float32)
    normed_heads = per_head * lax.rsqrt(lax.optimization_barrier(jnp.mean(per_head * per_head, axis=-1, keepdims=True)) + EPSILON) * head_gain
    gated = (normed_heads.reshape(n_tokens, -1) * jax.nn.silu(out_gate.reshape(n_tokens, -1).astype(jnp.float32))).astype(jnp.bfloat16)
    resid = stream.reshape(n_tokens, model_width).astype(jnp.float32) + jnp.dot(gated.astype(jnp.float32), out_proj.astype(jnp.float32), preferred_element_type=jnp.float32)
    ffn_in = (resid * lax.rsqrt(lax.optimization_barrier(jnp.mean(resid * resid, axis=-1, keepdims=True)) + EPSILON) * ffn_gain).astype(jnp.bfloat16)
    n_rows = N_SP * N_DP * CAP
    flat_routes = routes.reshape(n_tokens, TOP)
    flat_weight = route_weight.reshape(n_tokens, TOP)
    group_width = FF // N_DP

    def one_expert(index):
        hits = flat_routes == index
        member = jnp.any(hits, axis=1).astype(jnp.int32)
        order = jnp.argsort(1 - member, stable=True)[:n_rows].astype(jnp.int32)
        picked = ffn_in[order]
        share = lax.optimization_barrier(jnp.sum(jnp.where(hits, flat_weight, 0.0), axis=1))[order]
        gate_act = jnp.dot(picked.astype(jnp.float32), expert_gate[index].astype(jnp.float32), preferred_element_type=jnp.float32)
        up_act = jnp.dot(picked.astype(jnp.float32), expert_up[index].astype(jnp.float32), preferred_element_type=jnp.float32)
        hidden = (jax.nn.silu(gate_act) * up_act).astype(jnp.bfloat16)
        pieces = jnp.einsum('rpf,pfd->prd', hidden.reshape(n_rows, N_DP, group_width).astype(jnp.float32), expert_down[index].reshape(N_DP, group_width, model_width).astype(jnp.float32))
        rounded = lax.optimization_barrier(pieces.astype(jnp.bfloat16))
        expert_out = lax.optimization_barrier(jnp.sum(rounded.astype(jnp.float32), axis=0)).astype(jnp.bfloat16)
        return (order, expert_out.astype(jnp.float32) * share[:, None])
    orders, contribs = lax.map(one_expert, jnp.arange(EXPERTS, dtype=jnp.int32))
    routed = jax.ops.segment_sum(contribs.reshape(-1, model_width), orders.reshape(-1), num_segments=n_tokens)
    return (resid + routed).astype(jnp.bfloat16).reshape(stream.shape)
```

```python
import jax
import jax.numpy as jnp
from jax import lax
from jax.experimental import pallas as pl
from jax.experimental.pallas import tpu as pltpu
from jax.sharding import PartitionSpec as P

EPSILON = 1e-6
HEAD_DIM = 128
TOK = 128
BASE = 16
UNROLL = 2


def mm(a, b):
    return jnp.dot(a, b, preferred_element_type=jnp.float32)


def halves(a):
    high = a.astype(jnp.bfloat16)
    return high, (a - high.astype(jnp.float32)).astype(jnp.bfloat16)


def mm3(a, b):
    ah, al = halves(a)
    bh, bl = halves(b)
    return mm(ah, bh) + (mm(ah, bl) + mm(al, bh))


def unit_lower_inverse(low, rows, cols):
    n = low.shape[0]
    group = cols[:BASE] // BASE
    packed = jnp.where(group == 0, low[:BASE], 0.0)
    for b in range(1, n // BASE):
        packed = packed + jnp.where(group == b, low[b * BASE : (b + 1) * BASE], 0.0)
    inv = jnp.where(rows[:BASE] == cols[:BASE] % BASE, 1.0, 0.0)
    for j in range(BASE - 1):
        column = jnp.take_along_axis(packed, group * BASE + j, axis=1)
        inv = inv - column * inv[j : j + 1]
    full = jnp.concatenate([jnp.where(group == b, inv, 0.0) for b in range(n // BASE)], axis=0)
    width = BASE
    while width < n:
        off = (rows // (2 * width) == cols // (2 * width)) & (rows // width != cols // width)
        full = full - mm3(full, mm3(jnp.where(off, low, 0.0), full))
        width *= 2
    return full


def mixer_kernel(recv_ref, rate_ref, out_ref, vec_ref, step_ref, add_ref, acc_ref):
    n_blk = recv_ref.shape[0]
    rows = lax.broadcasted_iota(jnp.int32, (TOK, TOK), 0)
    cols = lax.broadcasted_iota(jnp.int32, (TOK, TOK), 1)
    rate = rate_ref[...]
    before = jnp.where(rows <= cols, 1.0, 0.0)
    after = jnp.where(rows >= cols, 1.0, 0.0)
    fwd_sum = jnp.dot(rate, before, precision=lax.Precision.HIGHEST, preferred_element_type=jnp.float32)
    bwd_sum = jnp.dot(rate, after, precision=lax.Precision.HIGHEST, preferred_element_type=jnp.float32)
    for n in range(n_blk):
        logit = recv_ref[n, 3 * TOK : 3 * TOK + 16, :].astype(jnp.float32)[0:1]
        vec_ref[n, 0:1, :] = fwd_sum[n : n + 1]
        vec_ref[n, 1:2, :] = bwd_sum[n : n + 1]
        vec_ref[n, 2:3, :] = jax.nn.sigmoid(logit)
        vec_ref[n, 3:4, :] = jnp.broadcast_to(fwd_sum[n : n + 1, TOK - 1 : TOK], (1, TOK))
        vec_ref[n, 4:8, :] = jnp.zeros((4, TOK), jnp.float32)

    def prepare(n):
        query = recv_ref[n, 0:TOK, :]
        key = recv_ref[n, TOK : 2 * TOK, :]
        query_f = query.astype(jnp.float32)
        key_f = key.astype(jnp.float32)
        value_f = recv_ref[n, 2 * TOK : 3 * TOK, :].astype(jnp.float32)
        key_tf = key_f.T
        key_t = key_tf.astype(jnp.bfloat16)
        key_c = lax.rsqrt(jnp.sum(key_f * key_f, axis=1, keepdims=True) + EPSILON)
        key_r = lax.rsqrt(jnp.sum(key_tf * key_tf, axis=0, keepdims=True) + EPSILON)
        query_c = lax.rsqrt(jnp.sum(query_f * query_f, axis=1, keepdims=True) + EPSILON) * HEAD_DIM ** (-0.5)
        vec_r = vec_ref[n]
        vec_c = vec_r.T
        beta_r, beta_c = vec_r[2:3], vec_c[:, 2:3]
        total = vec_r[3:4]
        kk = mm(key, key_t) * key_c * key_r
        qk = mm(query, key_t) * query_c * key_r
        acc = None
        for d in range(2):
            sum_r, sum_c = vec_r[d : d + 1], vec_c[:, d : d + 1]
            gap = sum_c - sum_r
            if d == 0:
                decay = jnp.exp(jnp.where(rows >= cols, gap, -jnp.inf))
                low = jnp.where(rows > cols, kk * decay, 0.0) * beta_c
                solve = unit_lower_inverse(low, rows, cols)
            else:
                decay = jnp.exp(jnp.where(rows <= cols, gap, -jnp.inf))
                low = jnp.where(rows > cols, kk * jnp.exp(jnp.where(rows >= cols, -gap, -jnp.inf)), 0.0) * beta_r
                solve = unit_lower_inverse(low, rows, cols).T
            grown = jnp.exp(sum_c)
            rhs = jnp.concatenate([value_f * beta_c, key_f * (beta_c * key_c * grown)], axis=1)
            both = mm(solve.astype(jnp.bfloat16), rhs.astype(jnp.bfloat16)).astype(jnp.bfloat16)
            lhs = jnp.concatenate([qk * decay, key_tf * (key_r * jnp.exp(total - sum_r))], axis=0)
            done = mm(lhs.astype(jnp.bfloat16), both)
            step_ref[d, n, 0:TOK, :] = (query_f * (query_c * grown) - done[:TOK, HEAD_DIM:]).astype(jnp.bfloat16)
            step_ref[d, n, TOK:, :] = done[TOK:, HEAD_DIM:].astype(jnp.bfloat16)
            add_ref[d, n] = done[TOK:, :HEAD_DIM]
            acc = done[:TOK, :HEAD_DIM] if acc is None else acc + done[:TOK, :HEAD_DIM]
        acc_ref[n] = acc

    def prepare_group(i, carry):
        for u in range(UNROLL):
            prepare(i * UNROLL + u)
        return carry

    lax.fori_loop(0, n_blk // UNROLL, prepare_group, 0)

    def walk(t, states):
        after_step = []
        for d, state in enumerate(states):
            n = t if d == 0 else n_blk - 1 - t
            high, low = halves(state)
            got = mm(step_ref[d, n], jnp.concatenate([high, low], axis=1))
            got = got[:, :HEAD_DIM] + got[:, HEAD_DIM:]
            acc_ref[n] = acc_ref[n] + got[:TOK]
            keep = jnp.exp(vec_ref[n][3:4])
            after_step.append(state * keep - got[TOK:] + add_ref[d, n])
        return tuple(after_step)

    zero = jnp.zeros((HEAD_DIM, HEAD_DIM), jnp.float32)
    lax.fori_loop(0, n_blk, walk, (zero, zero))
    out_ref[...] = acc_ref[...].astype(jnp.bfloat16)


def mixer(recv, rate, interpret=False):
    n_blk = recv.shape[0]
    return pl.pallas_call(
        mixer_kernel,
        out_shape=jax.ShapeDtypeStruct((n_blk, TOK, HEAD_DIM), jnp.bfloat16),
        in_specs=[pl.BlockSpec(memory_space=pltpu.VMEM)] * 2,
        out_specs=pl.BlockSpec(memory_space=pltpu.VMEM),
        scratch_shapes=[
            pltpu.VMEM((n_blk, 8, TOK), jnp.float32),
            pltpu.VMEM((2, n_blk, 2 * TOK, HEAD_DIM), jnp.bfloat16),
            pltpu.VMEM((2, n_blk, HEAD_DIM, HEAD_DIM), jnp.float32),
            pltpu.VMEM((n_blk, TOK, HEAD_DIM), jnp.float32),
        ],
        name="mixer",
        interpret=interpret,
    )(recv, rate)


def expert_part(rows, gate_local, up_local, down_local):
    gate_act = jnp.dot(rows, gate_local, preferred_element_type=jnp.float32)
    up_act = jnp.dot(rows, up_local, preferred_element_type=jnp.float32)
    hidden = (jax.nn.silu(gate_act) * up_act).astype(jnp.bfloat16)
    return jnp.dot(hidden, down_local, preferred_element_type=jnp.float32)


def body(
    stream,
    query_proj,
    key_proj,
    value_proj,
    out_gate,
    beta_logit,
    log_decay,
    head_gain,
    out_proj,
    ffn_gain,
    routes,
    route_weight,
    expert_gate,
    expert_up,
    expert_down,
):
    tok_count = stream.shape[1]
    model_width = stream.shape[2]
    n_heads = beta_logit.shape[2]

    def by_head(tensor):
        return tensor[0].reshape(tok_count, n_heads, HEAD_DIM).transpose(1, 0, 2)

    logits = jnp.pad(beta_logit[0].T[:, None, :], ((0, 0), (0, 15), (0, 0)))
    payload = jnp.concatenate(
        [by_head(query_proj), by_head(key_proj), by_head(value_proj), logits], axis=1
    )
    received = lax.all_to_all(payload, "sp", split_axis=0, concat_axis=0, tiled=True)
    mixed = mixer(received, log_decay.reshape(-1, TOK))
    tokens_view = lax.all_to_all(mixed, "sp", split_axis=0, concat_axis=0, tiled=True)
    per_head = tokens_view.astype(jnp.float32)
    normed_heads = (
        per_head
        * lax.rsqrt(jnp.mean(per_head * per_head, axis=-1, keepdims=True) + EPSILON)
        * head_gain
    )
    gated = (
        normed_heads.transpose(1, 0, 2).reshape(tok_count, -1) * jax.nn.silu(out_gate[0].astype(jnp.float32))
    ).astype(jnp.bfloat16)
    resid = stream[0].astype(jnp.float32) + jnp.dot(
        gated, out_proj, preferred_element_type=jnp.float32
    )
    ffn_in = (
        resid * lax.rsqrt(jnp.mean(resid * resid, axis=-1, keepdims=True) + EPSILON) * ffn_gain
    ).astype(jnp.bfloat16)
    n_sp = lax.axis_size("sp")
    top_count = routes.shape[2]
    capacity = tok_count * top_count * 2 // n_sp
    flat_routes = routes.reshape(-1)
    expert_ids = lax.broadcasted_iota(jnp.int32, (1, n_sp), 1)
    chosen = (flat_routes[:, None] == expert_ids).astype(jnp.int32)
    earlier = jnp.cumsum(chosen, axis=0) - chosen
    slot_ids = flat_routes * capacity + jnp.sum(earlier * chosen, axis=1)
    slot_grid = lax.broadcasted_iota(jnp.int32, (n_sp * capacity, 1), 0)
    placing = (
        (slot_grid == slot_ids[None, :])
        .astype(jnp.int32)
        .reshape(n_sp * capacity, tok_count, top_count)
    )
    placing = jnp.sum(placing, axis=2).astype(jnp.bfloat16)
    outgoing = jnp.dot(placing, ffn_in, preferred_element_type=jnp.float32).astype(jnp.bfloat16)
    outgoing = outgoing.reshape(n_sp, capacity, model_width)
    gate_local = expert_gate[0]
    up_local = expert_up[0]
    down_local = expert_down[0]
    arrived = lax.all_to_all(outgoing, "sp", split_axis=0, concat_axis=0, tiled=True)
    piece = lax.all_gather(arrived, "dp", axis=0, tiled=True)
    flat_rows = piece.reshape(-1, model_width)
    partial_value = expert_part(flat_rows, gate_local, up_local, down_local).reshape(
        piece.shape[0], piece.shape[1], model_width
    )
    summed = lax.psum_scatter(
        partial_value.astype(jnp.bfloat16), "dp", scatter_dimension=0, tiled=True
    )
    returned = lax.all_to_all(summed, "sp", split_axis=0, concat_axis=0, tiled=True)
    picked = returned.reshape(n_sp * capacity, model_width)[slot_ids]
    picked = picked.reshape(tok_count, top_count, model_width).astype(jnp.float32)
    routed = jnp.sum(picked * route_weight[0][..., None], axis=1)
    return (resid + routed).astype(jnp.bfloat16)[None]


def solution(mesh):
    return jax.shard_map(
        body,
        mesh=mesh,
        in_specs=(
            P("dp", "sp", None),
            P("dp", "sp", None),
            P("dp", "sp", None),
            P("dp", "sp", None),
            P("dp", "sp", None),
            P("dp", "sp", None),
            P("dp", "sp", None),
            P(),
            P(),
            P(),
            P("dp", "sp", None),
            P("dp", "sp", None),
            P("sp", None, "dp"),
            P("sp", None, "dp"),
            P("sp", "dp", None),
        ),
        out_specs=P("dp", "sp", None),
        check_vma=False,
    )
```

```python
import jax
import jax.numpy as jnp
from jax import lax
from jax.experimental import pallas as pl
from jax.experimental.pallas import tpu as pltpu
from jax.sharding import PartitionSpec as P

EPSILON = 1e-6
HEAD_DIM = 128
TOK = 128
BASE = 16
UNROLL = 2


def mm(a, b):
    return jnp.dot(a, b, preferred_element_type=jnp.float32)


def halves(a):
    high = a.astype(jnp.bfloat16)
    return high, (a - high.astype(jnp.float32)).astype(jnp.bfloat16)


def mm3(a, b):
    ah, al = halves(a)
    bh, bl = halves(b)
    return mm(ah, bh) + (mm(ah, bl) + mm(al, bh))


def unit_lower_inverse(low, rows, cols):
    n = low.shape[0]
    group = cols[:BASE] // BASE
    packed = jnp.where(group == 0, low[:BASE], 0.0)
    for b in range(1, n // BASE):
        packed = packed + jnp.where(group == b, low[b * BASE : (b + 1) * BASE], 0.0)
    inv = jnp.where(rows[:BASE] == cols[:BASE] % BASE, 1.0, 0.0)
    for j in range(BASE - 1):
        column = jnp.take_along_axis(packed, group * BASE + j, axis=1)
        inv = inv - column * inv[j : j + 1]
    full = jnp.concatenate([jnp.where(group == b, inv, 0.0) for b in range(n // BASE)], axis=0)
    width = BASE
    while width < n:
        off = (rows // (2 * width) == cols // (2 * width)) & (rows // width != cols // width)
        full = full - mm3(full, mm3(jnp.where(off, low, 0.0), full))
        width *= 2
    return full


def mixer_kernel(recv_ref, rate_ref, out_ref, vec_ref, step_ref, add_ref, acc_ref):
    n_blk = recv_ref.shape[0]
    rows = lax.broadcasted_iota(jnp.int32, (TOK, TOK), 0)
    cols = lax.broadcasted_iota(jnp.int32, (TOK, TOK), 1)
    rate = rate_ref[...]
    before = jnp.where(rows <= cols, 1.0, 0.0)
    after = jnp.where(rows >= cols, 1.0, 0.0)
    fwd_sum = jnp.dot(rate, before, precision=lax.Precision.HIGHEST, preferred_element_type=jnp.float32)
    bwd_sum = jnp.dot(rate, after, precision=lax.Precision.HIGHEST, preferred_element_type=jnp.float32)
    for n in range(n_blk):
        logit = recv_ref[n, 3 * TOK : 3 * TOK + 16, :].astype(jnp.float32)[0:1]
        vec_ref[n, 0:1, :] = fwd_sum[n : n + 1]
        vec_ref[n, 1:2, :] = bwd_sum[n : n + 1]
        vec_ref[n, 2:3, :] = jax.nn.sigmoid(logit)
        vec_ref[n, 3:4, :] = jnp.broadcast_to(fwd_sum[n : n + 1, TOK - 1 : TOK], (1, TOK))
        vec_ref[n, 4:8, :] = jnp.zeros((4, TOK), jnp.float32)

    def prepare(n):
        query = recv_ref[n, 0:TOK, :]
        key = recv_ref[n, TOK : 2 * TOK, :]
        query_f = query.astype(jnp.float32)
        key_f = key.astype(jnp.float32)
        value_f = recv_ref[n, 2 * TOK : 3 * TOK, :].astype(jnp.float32)
        key_tf = key_f.T
        key_t = key_tf.astype(jnp.bfloat16)
        key_c = lax.rsqrt(jnp.sum(key_f * key_f, axis=1, keepdims=True) + EPSILON)
        key_r = lax.rsqrt(jnp.sum(key_tf * key_tf, axis=0, keepdims=True) + EPSILON)
        query_c = lax.rsqrt(jnp.sum(query_f * query_f, axis=1, keepdims=True) + EPSILON) * HEAD_DIM ** (-0.5)
        vec_r = vec_ref[n]
        vec_c = vec_r.T
        beta_r, beta_c = vec_r[2:3], vec_c[:, 2:3]
        total = vec_r[3:4]
        kk = mm(key, key_t) * key_c * key_r
        qk = mm(query, key_t) * query_c * key_r
        acc = None
        for d in range(2):
            sum_r, sum_c = vec_r[d : d + 1], vec_c[:, d : d + 1]
            gap = sum_c - sum_r
            if d == 0:
                decay = jnp.exp(jnp.where(rows >= cols, gap, -jnp.inf))
                low = jnp.where(rows > cols, kk * decay, 0.0) * beta_c
                solve = unit_lower_inverse(low, rows, cols)
            else:
                decay = jnp.exp(jnp.where(rows <= cols, gap, -jnp.inf))
                low = jnp.where(rows > cols, kk * jnp.exp(jnp.where(rows >= cols, -gap, -jnp.inf)), 0.0) * beta_r
                solve = unit_lower_inverse(low, rows, cols).T
            grown = jnp.exp(sum_c)
            rhs = jnp.concatenate([value_f * beta_c, key_f * (beta_c * key_c * grown)], axis=1)
            both = mm(solve.astype(jnp.bfloat16), rhs.astype(jnp.bfloat16)).astype(jnp.bfloat16)
            lhs = jnp.concatenate([qk * decay, key_tf * (key_r * jnp.exp(total - sum_r))], axis=0)
            done = mm(lhs.astype(jnp.bfloat16), both)
            step_ref[d, n, 0:TOK, :] = (query_f * (query_c * grown) - done[:TOK, HEAD_DIM:]).astype(jnp.bfloat16)
            step_ref[d, n, TOK:, :] = done[TOK:, HEAD_DIM:].astype(jnp.bfloat16)
            add_ref[d, n] = done[TOK:, :HEAD_DIM]
            acc = done[:TOK, :HEAD_DIM] if acc is None else acc + done[:TOK, :HEAD_DIM]
        acc_ref[n] = acc

    def prepare_group(i, carry):
        for u in range(UNROLL):
            prepare(i * UNROLL + u)
        return carry

    lax.fori_loop(0, n_blk // UNROLL, prepare_group, 0)

    def walk(t, states):
        after_step = []
        for d, state in enumerate(states):
            n = t if d == 0 else n_blk - 1 - t
            high, low = halves(state)
            got = mm(step_ref[d, n], jnp.concatenate([high, low], axis=1))
            got = got[:, :HEAD_DIM] + got[:, HEAD_DIM:]
            acc_ref[n] = acc_ref[n] + got[:TOK]
            keep = jnp.exp(vec_ref[n][3:4])
            after_step.append(state * keep - got[TOK:] + add_ref[d, n])
        return tuple(after_step)

    zero = jnp.zeros((HEAD_DIM, HEAD_DIM), jnp.float32)
    lax.fori_loop(0, n_blk, walk, (zero, zero))
    out_ref[...] = acc_ref[...].astype(jnp.bfloat16)


def in_vmem(count):
    return [pl.BlockSpec(memory_space=pltpu.VMEM)] * count


def mixer(recv, rate):
    n_blk = recv.shape[0]
    return pl.pallas_call(
        mixer_kernel,
        out_shape=jax.ShapeDtypeStruct((n_blk, TOK, HEAD_DIM), jnp.bfloat16),
        in_specs=in_vmem(2),
        out_specs=in_vmem(1)[0],
        scratch_shapes=[
            pltpu.VMEM((n_blk, 8, TOK), jnp.float32),
            pltpu.VMEM((2, n_blk, 2 * TOK, HEAD_DIM), jnp.bfloat16),
            pltpu.VMEM((2, n_blk, HEAD_DIM, HEAD_DIM), jnp.float32),
            pltpu.VMEM((n_blk, TOK, HEAD_DIM), jnp.float32),
        ],
        compiler_params=pltpu.CompilerParams(vmem_limit_bytes=24 << 20),
        cost_estimate=pl.CostEstimate(flops=20 * 10**9, bytes_accessed=3 << 20, transcendentals=0),
        name="mixer",
    )(recv, rate)


def pack_kernel(query_ref, key_ref, value_ref, logit_ref, out_ref):
    logits = logit_ref[0].astype(jnp.float32).T.astype(jnp.bfloat16)
    for h in range(out_ref.shape[0]):
        lanes = slice(h * HEAD_DIM, (h + 1) * HEAD_DIM)
        out_ref[h, 0:TOK, :] = query_ref[0, :, lanes]
        out_ref[h, TOK : 2 * TOK, :] = key_ref[0, :, lanes]
        out_ref[h, 2 * TOK : 3 * TOK, :] = value_ref[0, :, lanes]
        out_ref[h, 3 * TOK :, :] = jnp.broadcast_to(logits[h : h + 1], (16, TOK))


def packed_heads(query_proj, key_proj, value_proj, beta_logit):
    n_heads = beta_logit.shape[2]
    return pl.pallas_call(
        pack_kernel,
        out_shape=jax.ShapeDtypeStruct((n_heads, 3 * TOK + 16, HEAD_DIM), jnp.bfloat16),
        in_specs=in_vmem(4),
        out_specs=in_vmem(1)[0],
        compiler_params=pltpu.CompilerParams(vmem_limit_bytes=16 << 20),
        cost_estimate=pl.CostEstimate(flops=10**6, bytes_accessed=3 << 20, transcendentals=0),
        name="pack",
    )(query_proj, key_proj, value_proj, beta_logit)


def expert_kernel(*refs, n_rows, n_parts):
    rows, refs = refs[:n_rows], refs[n_rows:]
    weights, refs = refs[: 3 * n_parts], refs[3 * n_parts :]
    outs, refs = refs[:n_rows], refs[n_rows:]
    bufs, accs, sems = refs[:3], refs[3 : 3 + n_rows], refs[3 + n_rows]
    for s in range(n_parts):
        for k in range(3):
            pltpu.make_async_copy(weights[3 * s + k], bufs[k].at[s], sems.at[k, s]).start()
    for acc in accs:
        acc[...] = jnp.zeros(acc.shape, jnp.float32)

    def part(s, carry):
        for k in range(3):
            pltpu.make_async_copy(weights[k], bufs[k].at[s], sems.at[k, s]).wait()
        for r in range(n_rows):
            gate_act = mm(rows[r][...], bufs[0][s])
            up_act = mm(rows[r][...], bufs[1][s])
            hidden = (jax.nn.silu(gate_act) * up_act).astype(jnp.bfloat16)
            accs[r][...] += mm(hidden, bufs[2][s])
        return carry

    lax.fori_loop(0, n_parts, part, 0)
    for acc, out in zip(accs, outs):
        out[...] = acc[...].astype(jnp.bfloat16)


def expert_part(rows, weights):
    n_parts = len(weights)
    count = sum(r.shape[0] for r in rows)
    width, units = weights[0][0].shape
    flat = [w for part in weights for w in part]
    return pl.pallas_call(
        lambda *refs: expert_kernel(*refs, n_rows=len(rows), n_parts=n_parts),
        out_shape=[jax.ShapeDtypeStruct(r.shape, jnp.bfloat16) for r in rows],
        in_specs=in_vmem(len(rows)) + [pl.BlockSpec(memory_space=pl.ANY)] * len(flat),
        out_specs=in_vmem(len(rows)),
        scratch_shapes=[pltpu.VMEM((n_parts, *w.shape), jnp.bfloat16) for w in weights[0]]
        + [pltpu.VMEM(r.shape, jnp.float32) for r in rows]
        + [pltpu.SemaphoreType.DMA((3, n_parts))],
        compiler_params=pltpu.CompilerParams(vmem_limit_bytes=52 << 20),
        cost_estimate=pl.CostEstimate(
            flops=6 * count * width * units * n_parts,
            bytes_accessed=6 * width * units * n_parts,
            transcendentals=0,
        ),
    )(*rows, *flat)


CHUNKS = 2


def body(
    stream,
    query_proj,
    key_proj,
    value_proj,
    out_gate,
    beta_logit,
    log_decay,
    head_gain,
    out_proj,
    ffn_gain,
    routes,
    route_weight,
    expert_gate,
    expert_up,
    expert_down,
):
    n_sp, n_dp = lax.axis_size("sp"), lax.axis_size("dp")
    tok_count, model_width = stream.shape[1:]
    chips = n_dp // 2
    to_neighbour = []
    for x in range(chips):
        to_neighbour.append((2 * ((x + 1) % chips), 2 * x))
        to_neighbour.append((2 * ((x - 1) % chips) + 1, 2 * x + 1))
    to_core = [(i, i ^ 1) for i in range(n_dp)]
    to_partner = [(i, (i + n_dp // 2) % n_dp) for i in range(n_dp)]

    def over_sp(tensor):
        return lax.all_to_all(tensor, "sp", split_axis=0, concat_axis=0, tiled=True)

    own = (expert_gate[0], expert_up[0], expert_down[0])
    near = tuple(lax.ppermute(w, "dp", to_core) for w in own)
    far = tuple(lax.ppermute(w, "dp", to_neighbour) for w in own)
    last = tuple(lax.ppermute(w, "dp", to_core) for w in far)
    weights = (own, near, far, last)

    received = over_sp(packed_heads(query_proj, key_proj, value_proj, beta_logit))
    mixed = mixer(received, log_decay.reshape(-1, TOK))
    per_head = over_sp(mixed).astype(jnp.float32)
    normed_heads = (
        per_head
        * lax.rsqrt(jnp.mean(per_head * per_head, axis=-1, keepdims=True) + EPSILON)
        * head_gain
    )
    gated = (
        normed_heads.transpose(1, 0, 2).reshape(tok_count, -1)
        * jax.nn.silu(out_gate[0].astype(jnp.float32))
    ).astype(jnp.bfloat16)
    resid = stream[0].astype(jnp.float32) + jnp.dot(
        gated, out_proj, preferred_element_type=jnp.float32
    )
    ffn_in = (
        resid * lax.rsqrt(jnp.mean(resid * resid, axis=-1, keepdims=True) + EPSILON) * ffn_gain
    ).astype(jnp.bfloat16)

    top_count = routes.shape[2]
    capacity = tok_count * top_count * 2 // n_sp
    piece = capacity // CHUNKS
    flat_routes = routes.reshape(-1)
    expert_ids = lax.broadcasted_iota(jnp.int32, (1, n_sp), 1)
    chosen = (flat_routes[:, None] == expert_ids).astype(jnp.int32)
    earlier = jnp.cumsum(chosen, axis=0) - chosen
    place = jnp.sum(earlier * chosen, axis=1)
    slot_ids = (place // piece) * (n_sp * piece) + flat_routes * piece + place % piece
    slot_grid = lax.broadcasted_iota(jnp.int32, (n_sp * capacity, 1, 1), 0)
    here = slot_grid == slot_ids.reshape(1, tok_count, top_count)
    placing = jnp.sum(here.astype(jnp.int32), axis=2).astype(jnp.bfloat16)
    share = jnp.sum(jnp.where(here, route_weight, 0.0), axis=2).T
    share_high, share_low = halves(share)
    outgoing = jnp.dot(placing, ffn_in, preferred_element_type=jnp.float32).astype(jnp.bfloat16)
    outgoing = outgoing.reshape(CHUNKS, n_sp, piece, model_width)

    mine, theirs = [], []
    for c in range(CHUNKS):
        arrived = over_sp(outgoing[c])
        mine.append(arrived.reshape(-1, model_width))
        theirs.append(lax.ppermute(arrived, "dp", to_partner).reshape(-1, model_width))
    kept = expert_part(mine, weights)
    result = resid
    for c in range(CHUNKS):
        (lent,) = expert_part([theirs[c]], weights)
        back = lax.ppermute(lent, "dp", to_partner)
        whole = (kept[c].astype(jnp.float32) + back.astype(jnp.float32)).astype(jnp.bfloat16)
        home = over_sp(whole.reshape(n_sp, piece, model_width)).reshape(-1, model_width)
        span = slice(c * n_sp * piece, (c + 1) * n_sp * piece)
        result = result + mm(share_high[:, span], home) + mm(share_low[:, span], home)
    return result.astype(jnp.bfloat16)[None]


def solution(mesh):
    return jax.shard_map(
        body,
        mesh=mesh,
        in_specs=(
            P("dp", "sp", None),
            P("dp", "sp", None),
            P("dp", "sp", None),
            P("dp", "sp", None),
            P("dp", "sp", None),
            P("dp", "sp", None),
            P("dp", "sp", None),
            P(),
            P(),
            P(),
            P("dp", "sp", None),
            P("dp", "sp", None),
            P("sp", None, "dp"),
            P("sp", None, "dp"),
            P("sp", "dp", None),
        ),
        out_specs=P("dp", "sp", None),
        check_vma=False,
    )
```

```python
import jax
import jax.numpy as jnp
from jax import lax
from jax.experimental import pallas as pl
from jax.experimental.pallas import tpu as pltpu
from jax.sharding import PartitionSpec as P

EPSILON = 1e-6
HEAD_DIM = 128
TOK = 128
BASE = 16
UNROLL = 4


def mm(a, b):
    return jnp.dot(a, b, preferred_element_type=jnp.float32)


def halves(a):
    high = a.astype(jnp.bfloat16)
    return high, (a - high.astype(jnp.float32)).astype(jnp.bfloat16)


def mm3(a, b):
    ah, al = halves(a)
    bh, bl = halves(b)
    return mm(ah, bh) + (mm(ah, bl) + mm(al, bh))


def unit_lower_inverses(lows, apart, cols):
    n = cols.shape[0]
    group = cols[:BASE] >> 4
    packs, invs = [], []
    for low in lows:
        packed = jnp.where(group == 0, low[:BASE], 0.0)
        for b in range(1, n // BASE):
            packed = packed + jnp.where(group == b, low[b * BASE : (b + 1) * BASE], 0.0)
        packs.append(packed)
        invs.append(jnp.where(apart[:BASE] & (BASE - 1) == 0, 1.0, 0.0))
    for j in range(BASE - 1):
        columns = [jnp.take_along_axis(packed, (group << 4) + j, axis=1) for packed in packs]
        invs = [inv - column * inv[j : j + 1] for inv, column in zip(invs, columns)]
    fulls = [
        jnp.concatenate([jnp.where(group == b, inv, 0.0) for b in range(n // BASE)], axis=0)
        for inv in invs
    ]
    for shift in range(4, n.bit_length() - 1):
        cross = apart >> shift == 1
        firsts = [mm3(jnp.where(cross, low, 0.0), full) for low, full in zip(lows, fulls)]
        seconds = [mm3(full, first) for full, first in zip(fulls, firsts)]
        fulls = [full - second for full, second in zip(fulls, seconds)]
    return fulls


def mixer_kernel(recv_ref, rate_ref, out_ref, vec_ref, step_ref, lhs_ref, add_ref, acc_ref):
    n_blk = recv_ref.shape[0]
    rows = lax.broadcasted_iota(jnp.int32, (TOK, TOK), 0)
    cols = lax.broadcasted_iota(jnp.int32, (TOK, TOK), 1)
    rate = rate_ref[...]
    before = jnp.where(rows <= cols, 1.0, 0.0)
    after = jnp.where(rows >= cols, 1.0, 0.0)
    fwd_sum = jnp.dot(rate, before, precision=lax.Precision.HIGHEST, preferred_element_type=jnp.float32)
    bwd_sum = jnp.dot(rate, after, precision=lax.Precision.HIGHEST, preferred_element_type=jnp.float32)
    for n in range(n_blk):
        logit = recv_ref[n, 3 * TOK : 3 * TOK + 16, :].astype(jnp.float32)[0:1]
        vec_ref[n, 0:1, :] = fwd_sum[n : n + 1]
        vec_ref[n, 1:2, :] = bwd_sum[n : n + 1]
        vec_ref[n, 2:3, :] = jax.nn.sigmoid(logit)
        vec_ref[n, 3:4, :] = jnp.broadcast_to(fwd_sum[n : n + 1, TOK - 1 : TOK], (1, TOK))
        vec_ref[n, 4:8, :] = jnp.zeros((4, TOK), jnp.float32)

    def prepare(blocks):
        made, lows = [], []
        for n in blocks:
            query = recv_ref[n, 0:TOK, :]
            key = recv_ref[n, TOK : 2 * TOK, :]
            query_f = query.astype(jnp.float32)
            key_f = key.astype(jnp.float32)
            key_tf = key_f.T
            key_t = key_tf.astype(jnp.bfloat16)
            key_c = lax.rsqrt(jnp.sum(key_f * key_f, axis=1, keepdims=True) + EPSILON)
            key_r = lax.rsqrt(jnp.sum(key_tf * key_tf, axis=0, keepdims=True) + EPSILON)
            query_c = lax.rsqrt(jnp.sum(query_f * query_f, axis=1, keepdims=True) + EPSILON)
            query_c = query_c * HEAD_DIM ** (-0.5)
            vec_r = vec_ref[n]
            vec_c = vec_r.T
            kk = mm(key, key_t) * key_c * key_r
            qk = mm(query, key_t) * query_c * key_r
            for d in range(2):
                sum_r, sum_c = vec_r[d : d + 1], vec_c[:, d : d + 1]
                gap = sum_c - sum_r
                if d == 0:
                    decay = jnp.exp(jnp.where(rows >= cols, gap, -jnp.inf))
                    lows.append(jnp.where(rows > cols, kk * decay, 0.0) * vec_c[:, 2:3])
                else:
                    decay = jnp.exp(jnp.where(rows <= cols, gap, -jnp.inf))
                    turned = jnp.exp(jnp.where(rows >= cols, -gap, -jnp.inf))
                    lows.append(jnp.where(rows > cols, kk * turned, 0.0) * vec_r[2:3])
                lhs_ref[d, n, 0:TOK, :] = (qk * decay).astype(jnp.bfloat16)
                tail = key_r * jnp.exp(vec_r[3:4] - sum_r)
                lhs_ref[d, n, TOK:, :] = (key_tf * tail).astype(jnp.bfloat16)
            made.append((key_c, query_c, vec_c))
        solves = unit_lower_inverses(lows, rows ^ cols, cols)
        boths = []
        for i, n in enumerate(blocks):
            key_c, query_c, vec_c = made[i]
            beta_c = vec_c[:, 2:3]
            key_f = recv_ref[n, TOK : 2 * TOK, :].astype(jnp.float32)
            write = recv_ref[n, 2 * TOK : 3 * TOK, :].astype(jnp.float32) * beta_c
            for d in range(2):
                solve = solves[2 * i + d] if d == 0 else solves[2 * i + d].T
                grown = jnp.exp(vec_c[:, d : d + 1])
                rhs = jnp.concatenate([write, key_f * (beta_c * key_c * grown)], axis=1)
                boths.append(mm(solve.astype(jnp.bfloat16), rhs.astype(jnp.bfloat16)).astype(jnp.bfloat16))
        dones = [mm(lhs_ref[j % 2, blocks[j // 2]], both) for j, both in enumerate(boths)]
        for i, n in enumerate(blocks):
            key_c, query_c, vec_c = made[i]
            query_f = recv_ref[n, 0:TOK, :].astype(jnp.float32)
            for d in range(2):
                done = dones[2 * i + d]
                grown = query_c * jnp.exp(vec_c[:, d : d + 1])
                step_ref[d, n, 0:TOK, :] = (query_f * grown - done[:TOK, HEAD_DIM:]).astype(jnp.bfloat16)
                step_ref[d, n, TOK:, :] = done[TOK:, HEAD_DIM:].astype(jnp.bfloat16)
                add_ref[d, n] = done[TOK:, :HEAD_DIM]
            acc_ref[n] = dones[2 * i][:TOK, :HEAD_DIM] + dones[2 * i + 1][:TOK, :HEAD_DIM]

    def prepare_group(i, carry):
        prepare([i * UNROLL + u for u in range(UNROLL)])
        return carry

    lax.fori_loop(0, n_blk // UNROLL, prepare_group, 0)

    def walk(t, states):
        after_step = []
        for d, state in enumerate(states):
            n = t if d == 0 else n_blk - 1 - t
            high, low = halves(state)
            got = mm(step_ref[d, n], jnp.concatenate([high, low], axis=1))
            got = got[:, :HEAD_DIM] + got[:, HEAD_DIM:]
            acc_ref[n] = acc_ref[n] + got[:TOK]
            keep = jnp.exp(vec_ref[n][3:4])
            after_step.append(state * keep - got[TOK:] + add_ref[d, n])
        return tuple(after_step)

    zero = jnp.zeros((HEAD_DIM, HEAD_DIM), jnp.float32)
    lax.fori_loop(0, n_blk, walk, (zero, zero))
    out_ref[...] = acc_ref[...].astype(jnp.bfloat16)


def in_vmem(count):
    return [pl.BlockSpec(memory_space=pltpu.VMEM)] * count


def mixer(recv, rate):
    n_blk = recv.shape[0]
    return pl.pallas_call(
        mixer_kernel,
        out_shape=jax.ShapeDtypeStruct((n_blk, TOK, HEAD_DIM), jnp.bfloat16),
        in_specs=in_vmem(2),
        out_specs=in_vmem(1)[0],
        scratch_shapes=[
            pltpu.VMEM((n_blk, 8, TOK), jnp.float32),
            pltpu.VMEM((2, n_blk, 2 * TOK, HEAD_DIM), jnp.bfloat16),
            pltpu.VMEM((2, n_blk, 2 * TOK, HEAD_DIM), jnp.bfloat16),
            pltpu.VMEM((2, n_blk, HEAD_DIM, HEAD_DIM), jnp.float32),
            pltpu.VMEM((n_blk, TOK, HEAD_DIM), jnp.float32),
        ],
        compiler_params=pltpu.CompilerParams(vmem_limit_bytes=24 << 20),
        cost_estimate=pl.CostEstimate(flops=20 * 10**9, bytes_accessed=3 << 20, transcendentals=0),
        name="mixer",
    )(recv, rate)


def pack_kernel(query_ref, key_ref, value_ref, logit_ref, out_ref):
    logits = logit_ref[0].astype(jnp.float32).T.astype(jnp.bfloat16)
    for h in range(out_ref.shape[0]):
        lanes = slice(h * HEAD_DIM, (h + 1) * HEAD_DIM)
        out_ref[h, 0:TOK, :] = query_ref[0, :, lanes]
        out_ref[h, TOK : 2 * TOK, :] = key_ref[0, :, lanes]
        out_ref[h, 2 * TOK : 3 * TOK, :] = value_ref[0, :, lanes]
        out_ref[h, 3 * TOK :, :] = jnp.broadcast_to(logits[h : h + 1], (16, TOK))


def packed_heads(query_proj, key_proj, value_proj, beta_logit):
    n_heads = beta_logit.shape[2]
    return pl.pallas_call(
        pack_kernel,
        out_shape=jax.ShapeDtypeStruct((n_heads, 3 * TOK + 16, HEAD_DIM), jnp.bfloat16),
        in_specs=in_vmem(4),
        out_specs=in_vmem(1)[0],
        compiler_params=pltpu.CompilerParams(vmem_limit_bytes=16 << 20),
        cost_estimate=pl.CostEstimate(flops=10**6, bytes_accessed=3 << 20, transcendentals=0),
        name="pack",
    )(query_proj, key_proj, value_proj, beta_logit)


def expert_kernel(*refs, n_rows, n_parts, n_after):
    rows, refs = refs[:n_rows], refs[n_rows:]
    weights, refs = refs[: 3 * n_parts], refs[3 * n_parts + n_after :]
    outs, refs = refs[:n_rows], refs[n_rows:]
    bufs, accs, sems = refs[:3], refs[3 : 3 + n_rows], refs[3 + n_rows]
    for s in range(n_parts):
        for k in range(3):
            pltpu.make_async_copy(weights[3 * s + k], bufs[k].at[s], sems.at[k, s]).start()
    for acc in accs:
        acc[...] = jnp.zeros(acc.shape, jnp.float32)

    def part(s, carry):
        for k in range(3):
            pltpu.make_async_copy(weights[k], bufs[k].at[s], sems.at[k, s]).wait()
        for r in range(n_rows):
            gate_act = mm(rows[r][...], bufs[0][s])
            up_act = mm(rows[r][...], bufs[1][s])
            hidden = (jax.nn.silu(gate_act) * up_act).astype(jnp.bfloat16)
            accs[r][...] += mm(hidden, bufs[2][s])
        return carry

    lax.fori_loop(0, n_parts, part, 0)
    for acc, out in zip(accs, outs):
        out[...] = acc[...].astype(jnp.bfloat16)


def expert_part(rows, weights, after=()):
    n_parts = len(weights)
    count = sum(r.shape[0] for r in rows)
    width, units = weights[0][0].shape
    flat = [w for part in weights for w in part]
    return pl.pallas_call(
        lambda *refs: expert_kernel(*refs, n_rows=len(rows), n_parts=n_parts, n_after=len(after)),
        out_shape=[jax.ShapeDtypeStruct(r.shape, jnp.bfloat16) for r in rows],
        in_specs=in_vmem(len(rows)) + [pl.BlockSpec(memory_space=pltpu.HBM)] * (len(flat) + len(after)),
        out_specs=in_vmem(len(rows)),
        scratch_shapes=[pltpu.VMEM((n_parts, *w.shape), jnp.bfloat16) for w in weights[0]]
        + [pltpu.VMEM(r.shape, jnp.float32) for r in rows]
        + [pltpu.SemaphoreType.DMA((3, n_parts))],
        compiler_params=pltpu.CompilerParams(vmem_limit_bytes=52 << 20),
        cost_estimate=pl.CostEstimate(
            flops=6 * count * width * units * n_parts,
            bytes_accessed=6 * width * units * n_parts,
            transcendentals=0,
        ),
    )(*rows, *flat, *after)


def project_kernel(
    mixed_ref, gate_ref, stream_ref, head_gain_ref, proj_hbm, ffn_gain_ref, placing_ref, *refs
):
    *outs, resid_ref, gated_ref, proj_ref, sems = refs
    parts = sems.shape[0]
    deep = proj_ref.shape[0] // parts
    copies = []
    for k in range(parts):
        span = slice(k * deep, (k + 1) * deep)
        copies.append(
            pltpu.make_async_copy(proj_hbm.at[span, :], proj_ref.at[span, :], sems.at[k])
        )
        copies[-1].start()
    for h in range(mixed_ref.shape[0]):
        lanes = slice(h * HEAD_DIM, (h + 1) * HEAD_DIM)
        head = mixed_ref[h].astype(jnp.float32)
        scale = lax.rsqrt(jnp.mean(head * head, axis=1, keepdims=True) + EPSILON)
        gate = jax.nn.silu(gate_ref[0, :, lanes].astype(jnp.float32))
        gated_ref[:, lanes] = (head * scale * head_gain_ref[...] * gate).astype(jnp.bfloat16)
    resid = stream_ref[0].astype(jnp.float32)
    for k in range(parts):
        span = slice(k * deep, (k + 1) * deep)
        copies[k].wait()
        resid = resid + mm(gated_ref[:, span], proj_ref[span, :])
    resid_ref[...] = resid
    scale = lax.rsqrt(jnp.mean(resid * resid, axis=1, keepdims=True) + EPSILON)
    ffn_in = (resid * scale * ffn_gain_ref[...]).astype(jnp.bfloat16)
    at = 0
    for out in outs:
        out[...] = mm(placing_ref[at : at + out.shape[0], :], ffn_in).astype(jnp.bfloat16)
        at += out.shape[0]


def project(mixed, out_gate, stream, head_gain, out_proj, ffn_gain, placing, n_out):
    tok_count, model_width = stream.shape[1:]
    part = placing.shape[0] // n_out
    *outs, resid = pl.pallas_call(
        project_kernel,
        out_shape=[jax.ShapeDtypeStruct((part, model_width), jnp.bfloat16)] * n_out
        + [jax.ShapeDtypeStruct((tok_count, model_width), jnp.float32)],
        in_specs=in_vmem(4) + [pl.BlockSpec(memory_space=pltpu.HBM)] + in_vmem(2),
        out_specs=in_vmem(n_out + 1),
        scratch_shapes=[
            pltpu.VMEM((tok_count, model_width), jnp.bfloat16),
            pltpu.VMEM(out_proj.shape, jnp.bfloat16),
            pltpu.SemaphoreType.DMA((4,)),
        ],
        compiler_params=pltpu.CompilerParams(vmem_limit_bytes=32 << 20),
        cost_estimate=pl.CostEstimate(
            flops=3 * tok_count * model_width * model_width,
            bytes_accessed=2 * model_width * model_width,
            transcendentals=0,
        ),
        name="project",
    )(mixed, out_gate, stream, head_gain[None], out_proj, ffn_gain[None], placing)
    return outs, resid


CHUNKS = 2


def body(
    stream,
    query_proj,
    key_proj,
    value_proj,
    out_gate,
    beta_logit,
    log_decay,
    head_gain,
    out_proj,
    ffn_gain,
    routes,
    route_weight,
    expert_gate,
    expert_up,
    expert_down,
):
    n_sp, n_dp = lax.axis_size("sp"), lax.axis_size("dp")
    tok_count, model_width = stream.shape[1:]
    chips = n_dp // 2
    to_neighbour = []
    for x in range(chips):
        to_neighbour.append((2 * ((x + 1) % chips), 2 * x))
        to_neighbour.append((2 * ((x - 1) % chips) + 1, 2 * x + 1))
    to_core = [(i, i ^ 1) for i in range(n_dp)]
    to_partner = [(i, (i + n_dp // 2) % n_dp) for i in range(n_dp)]

    def over_sp(tensor):
        return lax.all_to_all(tensor, "sp", split_axis=0, concat_axis=0, tiled=True)

    own = (expert_gate[0], expert_up[0], expert_down[0])
    near = tuple(lax.ppermute(w, "dp", to_core) for w in own)
    far = tuple(lax.ppermute(w, "dp", to_neighbour) for w in own)
    received = over_sp(packed_heads(query_proj, key_proj, value_proj, beta_logit))
    mixed = mixer(received, log_decay.reshape(-1, TOK))
    top_count = routes.shape[2]
    capacity = tok_count * top_count * 2 // n_sp
    piece = capacity // CHUNKS
    flat_routes = routes.reshape(-1)
    expert_ids = lax.broadcasted_iota(jnp.int32, (1, n_sp), 1)
    chosen = (flat_routes[:, None] == expert_ids).astype(jnp.int32)
    earlier = jnp.cumsum(chosen, axis=0) - chosen
    place = jnp.sum(earlier * chosen, axis=1)
    slot_ids = (place // piece) * (n_sp * piece) + flat_routes * piece + place % piece
    slot_grid = lax.broadcasted_iota(jnp.int32, (n_sp * capacity, 1, 1), 0)
    here = slot_grid == slot_ids.reshape(1, tok_count, top_count)
    placing = jnp.sum(here.astype(jnp.int32), axis=2).astype(jnp.bfloat16)
    share = jnp.sum(jnp.where(here, route_weight, 0.0), axis=2).T
    share_high, share_low = halves(share)
    outgoing, resid = project(
        over_sp(mixed), out_gate, stream, head_gain, out_proj, ffn_gain, placing, CHUNKS
    )

    mine, theirs = [], []
    for c in range(CHUNKS):
        arrived = over_sp(outgoing[c].reshape(n_sp, piece, model_width))
        mine.append(arrived.reshape(-1, model_width))
        theirs.append(lax.ppermute(arrived, "dp", to_partner).reshape(-1, model_width))
        if c == 0:
            *far, mine[0] = lax.optimization_barrier((*far, mine[0]))
            last = tuple(lax.ppermute(w, "dp", to_core) for w in far)
    weights = (own, near, tuple(far), last)
    turns = [("mine", 0)] + [("theirs", c) for c in range(CHUNKS)]
    turns += [("mine", c) for c in range(1, CHUNKS)]
    made, before = {}, ()
    for side, c in turns:
        rows = mine[c] if side == "mine" else theirs[c]
        before = tuple(expert_part([rows], weights, before))
        made[side, c] = before[0]
    result = resid
    for c in range(CHUNKS):
        back = lax.ppermute(made["theirs", c], "dp", to_partner)
        whole = (made["mine", c].astype(jnp.float32) + back.astype(jnp.float32)).astype(jnp.bfloat16)
        home = over_sp(whole.reshape(n_sp, piece, model_width)).reshape(-1, model_width)
        span = slice(c * n_sp * piece, (c + 1) * n_sp * piece)
        result = result + mm(share_high[:, span], home) + mm(share_low[:, span], home)
    return result.astype(jnp.bfloat16)[None]


def solution(mesh):
    return jax.shard_map(
        body,
        mesh=mesh,
        in_specs=(
            P("dp", "sp", None),
            P("dp", "sp", None),
            P("dp", "sp", None),
            P("dp", "sp", None),
            P("dp", "sp", None),
            P("dp", "sp", None),
            P("dp", "sp", None),
            P(),
            P(),
            P(),
            P("dp", "sp", None),
            P("dp", "sp", None),
            P("sp", None, "dp"),
            P("sp", None, "dp"),
            P("sp", "dp", None),
        ),
        out_specs=P("dp", "sp", None),
        check_vma=False,
    )
```

```python
import jax
import jax.numpy as jnp
from jax import lax
from jax.experimental import pallas as pl
from jax.experimental.pallas import tpu as pltpu
from jax.sharding import PartitionSpec as P


EPSILON = 1e-6
HEAD_DIM = 128
TOK = 128
BASE = 16
UNROLL = 8


def mm(a, b):
    return jnp.dot(a, b, preferred_element_type=jnp.float32)


def halves(a):
    high = a.astype(jnp.bfloat16)
    return high, (a - high.astype(jnp.float32)).astype(jnp.bfloat16)


def mm3(a, b):
    ah, al = halves(a)
    bh, bl = halves(b)
    return mm(ah, bh) + (mm(ah, bl) + mm(al, bh))


def unit_lower_inverses(lows, apart, cols):
    n = cols.shape[0]
    group = cols[:BASE] >> 4
    packs, invs = [], []
    for low in lows:
        packed = jnp.where(group == 0, low[:BASE], 0.0)
        for b in range(1, n // BASE):
            packed = packed + jnp.where(group == b, low[b * BASE : (b + 1) * BASE], 0.0)
        packs.append(packed)
        invs.append(jnp.where(apart[:BASE] & (BASE - 1) == 0, 1.0, 0.0))
    for j in range(BASE - 1):
        columns = [jnp.take_along_axis(packed, (group << 4) + j, axis=1) for packed in packs]
        invs = [inv - column * inv[j : j + 1] for inv, column in zip(invs, columns)]
    fulls = [
        jnp.concatenate([jnp.where(group == b, inv, 0.0) for b in range(n // BASE)], axis=0)
        for inv in invs
    ]
    for shift in range(4, n.bit_length() - 1):
        cross = apart >> shift == 1
        firsts = [mm3(jnp.where(cross, low, 0.0), full) for low, full in zip(lows, fulls)]
        seconds = [mm3(full, first) for full, first in zip(fulls, firsts)]
        fulls = [full - second for full, second in zip(fulls, seconds)]
    return fulls


def mixer_kernel(recv_ref, rate_ref, out_ref, vec_ref, step_ref, lhs_ref, add_ref, acc_ref):
    n_blk = recv_ref.shape[0]
    rows = lax.broadcasted_iota(jnp.int32, (TOK, TOK), 0)
    cols = lax.broadcasted_iota(jnp.int32, (TOK, TOK), 1)
    rate = rate_ref[...]
    before = jnp.where(rows <= cols, 1.0, 0.0)
    after = jnp.where(rows >= cols, 1.0, 0.0)
    fwd_sum = jnp.dot(rate, before, precision=lax.Precision.HIGHEST, preferred_element_type=jnp.float32)
    bwd_sum = jnp.dot(rate, after, precision=lax.Precision.HIGHEST, preferred_element_type=jnp.float32)
    for n in range(n_blk):
        logit = recv_ref[n, 3 * TOK : 3 * TOK + 16, :].astype(jnp.float32)[0:1]
        vec_ref[n, 0:1, :] = fwd_sum[n : n + 1]
        vec_ref[n, 1:2, :] = bwd_sum[n : n + 1]
        vec_ref[n, 2:3, :] = jax.nn.sigmoid(logit)
        vec_ref[n, 3:4, :] = jnp.broadcast_to(fwd_sum[n : n + 1, TOK - 1 : TOK], (1, TOK))
        vec_ref[n, 4:8, :] = jnp.zeros((4, TOK), jnp.float32)

    def prepare(blocks):
        made, lows = [], []
        for n in blocks:
            query = recv_ref[n, 0:TOK, :]
            key = recv_ref[n, TOK : 2 * TOK, :]
            query_f = query.astype(jnp.float32)
            key_f = key.astype(jnp.float32)
            key_tf = key_f.T
            key_t = key_tf.astype(jnp.bfloat16)
            key_c = lax.rsqrt(jnp.sum(key_f * key_f, axis=1, keepdims=True) + EPSILON)
            key_r = lax.rsqrt(jnp.sum(key_tf * key_tf, axis=0, keepdims=True) + EPSILON)
            query_c = lax.rsqrt(jnp.sum(query_f * query_f, axis=1, keepdims=True) + EPSILON)
            query_c = query_c * HEAD_DIM ** (-0.5)
            vec_r = vec_ref[n]
            vec_c = vec_r.T
            kk = mm(key, key_t) * key_c * key_r
            qk = mm(query, key_t) * query_c * key_r
            for d in range(2):
                sum_r, sum_c = vec_r[d : d + 1], vec_c[:, d : d + 1]
                gap = sum_c - sum_r
                if d == 0:
                    decay = jnp.exp(jnp.where(rows >= cols, gap, -jnp.inf))
                    lows.append(jnp.where(rows > cols, kk * decay, 0.0) * vec_c[:, 2:3])
                else:
                    decay = jnp.exp(jnp.where(rows <= cols, gap, -jnp.inf))
                    turned = jnp.exp(jnp.where(rows >= cols, -gap, -jnp.inf))
                    lows.append(jnp.where(rows > cols, kk * turned, 0.0) * vec_r[2:3])
                lhs_ref[d, n, 0:TOK, :] = (qk * decay).astype(jnp.bfloat16)
                tail = key_r * jnp.exp(vec_r[3:4] - sum_r)
                lhs_ref[d, n, TOK:, :] = (key_tf * tail).astype(jnp.bfloat16)
            made.append((key_c, query_c, vec_c))
        solves = unit_lower_inverses(lows, rows ^ cols, cols)
        boths = []
        for i, n in enumerate(blocks):
            key_c, query_c, vec_c = made[i]
            beta_c = vec_c[:, 2:3]
            key_f = recv_ref[n, TOK : 2 * TOK, :].astype(jnp.float32)
            write = recv_ref[n, 2 * TOK : 3 * TOK, :].astype(jnp.float32) * beta_c
            for d in range(2):
                solve = solves[2 * i + d] if d == 0 else solves[2 * i + d].T
                grown = jnp.exp(vec_c[:, d : d + 1])
                rhs = jnp.concatenate([write, key_f * (beta_c * key_c * grown)], axis=1)
                boths.append(mm(solve.astype(jnp.bfloat16), rhs.astype(jnp.bfloat16)).astype(jnp.bfloat16))
        dones = [mm(lhs_ref[j % 2, blocks[j // 2]], both) for j, both in enumerate(boths)]
        for i, n in enumerate(blocks):
            key_c, query_c, vec_c = made[i]
            query_f = recv_ref[n, 0:TOK, :].astype(jnp.float32)
            for d in range(2):
                done = dones[2 * i + d]
                grown = query_c * jnp.exp(vec_c[:, d : d + 1])
                step_ref[d, n, 0:TOK, :] = (query_f * grown - done[:TOK, HEAD_DIM:]).astype(jnp.bfloat16)
                step_ref[d, n, TOK:, :] = done[TOK:, HEAD_DIM:].astype(jnp.bfloat16)
                add_ref[d, n] = done[TOK:, :HEAD_DIM]
            acc_ref[n] = dones[2 * i][:TOK, :HEAD_DIM] + dones[2 * i + 1][:TOK, :HEAD_DIM]

    def prepare_group(i, carry):
        prepare([i * UNROLL + u for u in range(UNROLL)])
        return carry

    lax.fori_loop(0, n_blk // UNROLL, prepare_group, 0)

    def walk(t, states):
        after_step = []
        for d, state in enumerate(states):
            n = t if d == 0 else n_blk - 1 - t
            high, low = halves(state)
            got = mm(step_ref[d, n], jnp.concatenate([high, low], axis=1))
            got = got[:, :HEAD_DIM] + got[:, HEAD_DIM:]
            acc_ref[n] = acc_ref[n] + got[:TOK]
            keep = jnp.exp(vec_ref[n][3:4])
            after_step.append(state * keep - got[TOK:] + add_ref[d, n])
        return tuple(after_step)

    zero = jnp.zeros((HEAD_DIM, HEAD_DIM), jnp.float32)
    lax.fori_loop(0, n_blk, walk, (zero, zero))
    out_ref[...] = acc_ref[...].astype(jnp.bfloat16)


def in_vmem(count):
    return [pl.BlockSpec(memory_space=pltpu.VMEM)] * count


def mixer(recv, rate):
    n_blk = recv.shape[0]
    return pl.pallas_call(
        mixer_kernel,
        out_shape=jax.ShapeDtypeStruct((n_blk, TOK, HEAD_DIM), jnp.bfloat16),
        in_specs=in_vmem(2),
        out_specs=in_vmem(1)[0],
        scratch_shapes=[
            pltpu.VMEM((n_blk, 8, TOK), jnp.float32),
            pltpu.VMEM((2, n_blk, 2 * TOK, HEAD_DIM), jnp.bfloat16),
            pltpu.VMEM((2, n_blk, 2 * TOK, HEAD_DIM), jnp.bfloat16),
            pltpu.VMEM((2, n_blk, HEAD_DIM, HEAD_DIM), jnp.float32),
            pltpu.VMEM((n_blk, TOK, HEAD_DIM), jnp.float32),
        ],
        compiler_params=pltpu.CompilerParams(vmem_limit_bytes=24 << 20),
        cost_estimate=pl.CostEstimate(flops=20 * 10**9, bytes_accessed=3 << 20, transcendentals=0),
        name="mixer",
    )(recv, rate)


def pack_kernel(query_ref, key_ref, value_ref, logit_ref, out_ref):
    logits = logit_ref[0].astype(jnp.float32).T.astype(jnp.bfloat16)
    for h in range(out_ref.shape[0]):
        lanes = slice(h * HEAD_DIM, (h + 1) * HEAD_DIM)
        out_ref[h, 0:TOK, :] = query_ref[0, :, lanes]
        out_ref[h, TOK : 2 * TOK, :] = key_ref[0, :, lanes]
        out_ref[h, 2 * TOK : 3 * TOK, :] = value_ref[0, :, lanes]
        out_ref[h, 3 * TOK :, :] = jnp.broadcast_to(logits[h : h + 1], (16, TOK))


def packed_heads(query_proj, key_proj, value_proj, beta_logit):
    n_heads = beta_logit.shape[2]
    return pl.pallas_call(
        pack_kernel,
        out_shape=jax.ShapeDtypeStruct((n_heads, 3 * TOK + 16, HEAD_DIM), jnp.bfloat16),
        in_specs=in_vmem(4),
        out_specs=in_vmem(1)[0],
        compiler_params=pltpu.CompilerParams(vmem_limit_bytes=16 << 20),
        cost_estimate=pl.CostEstimate(flops=10**6, bytes_accessed=3 << 20, transcendentals=0),
        name="pack",
    )(query_proj, key_proj, value_proj, beta_logit)


def expert_kernel(*refs, n_rows, n_parts, n_after):
    rows, refs = refs[:n_rows], refs[n_rows:]
    weights, refs = refs[: 3 * n_parts], refs[3 * n_parts + n_after :]
    outs, refs = refs[:n_rows], refs[n_rows:]
    bufs, accs, sems = refs[:3], refs[3 : 3 + n_rows], refs[3 + n_rows]
    for s in range(n_parts):
        for k in range(3):
            pltpu.make_async_copy(weights[3 * s + k], bufs[k].at[s], sems.at[k, s]).start()
    for acc in accs:
        acc[...] = jnp.zeros(acc.shape, jnp.float32)

    def part(s, carry):
        for k in range(3):
            pltpu.make_async_copy(weights[k], bufs[k].at[s], sems.at[k, s]).wait()
        for r in range(n_rows):
            gate_act = mm(rows[r][...], bufs[0][s])
            up_act = mm(rows[r][...], bufs[1][s])
            hidden = (jax.nn.silu(gate_act) * up_act).astype(jnp.bfloat16)
            accs[r][...] += mm(hidden, bufs[2][s])
        return carry

    lax.fori_loop(0, n_parts, part, 0)
    for acc, out in zip(accs, outs):
        out[...] = acc[...].astype(jnp.bfloat16)


def expert_part(rows, weights, after=()):
    n_parts = len(weights)
    count = sum(r.shape[0] for r in rows)
    width, units = weights[0][0].shape
    flat = [w for part in weights for w in part]
    return pl.pallas_call(
        lambda *refs: expert_kernel(*refs, n_rows=len(rows), n_parts=n_parts, n_after=len(after)),
        out_shape=[jax.ShapeDtypeStruct(r.shape, jnp.bfloat16) for r in rows],
        in_specs=in_vmem(len(rows)) + [pl.BlockSpec(memory_space=pltpu.HBM)] * (len(flat) + len(after)),
        out_specs=in_vmem(len(rows)),
        scratch_shapes=[pltpu.VMEM((n_parts, *w.shape), jnp.bfloat16) for w in weights[0]]
        + [pltpu.VMEM(r.shape, jnp.float32) for r in rows]
        + [pltpu.SemaphoreType.DMA((3, n_parts))],
        compiler_params=pltpu.CompilerParams(vmem_limit_bytes=52 << 20),
        cost_estimate=pl.CostEstimate(
            flops=6 * count * width * units * n_parts,
            bytes_accessed=6 * width * units * n_parts,
            transcendentals=0,
        ),
    )(*rows, *flat, *after)


def project_kernel(
    mixed_ref, gate_ref, stream_ref, head_gain_ref, proj_hbm, ffn_gain_ref, placing_ref, *refs
):
    *outs, resid_ref, gated_ref, proj_ref, sems = refs
    parts = sems.shape[0]
    deep = proj_ref.shape[0] // parts
    copies = []
    for k in range(parts):
        span = slice(k * deep, (k + 1) * deep)
        copies.append(
            pltpu.make_async_copy(proj_hbm.at[span, :], proj_ref.at[span, :], sems.at[k])
        )
        copies[-1].start()
    for h in range(mixed_ref.shape[0]):
        lanes = slice(h * HEAD_DIM, (h + 1) * HEAD_DIM)
        head = mixed_ref[h].astype(jnp.float32)
        scale = lax.rsqrt(jnp.mean(head * head, axis=1, keepdims=True) + EPSILON)
        gate = jax.nn.silu(gate_ref[0, :, lanes].astype(jnp.float32))
        gated_ref[:, lanes] = (head * scale * head_gain_ref[...] * gate).astype(jnp.bfloat16)
    resid = stream_ref[0].astype(jnp.float32)
    for k in range(parts):
        span = slice(k * deep, (k + 1) * deep)
        copies[k].wait()
        resid = resid + mm(gated_ref[:, span], proj_ref[span, :])
    resid_ref[...] = resid
    scale = lax.rsqrt(jnp.mean(resid * resid, axis=1, keepdims=True) + EPSILON)
    ffn_in = (resid * scale * ffn_gain_ref[...]).astype(jnp.bfloat16)
    at = 0
    for out in outs:
        out[...] = mm(placing_ref[at : at + out.shape[0], :], ffn_in).astype(jnp.bfloat16)
        at += out.shape[0]


def project(mixed, out_gate, stream, head_gain, out_proj, ffn_gain, placing, n_out):
    tok_count, model_width = stream.shape[1:]
    part = placing.shape[0] // n_out
    *outs, resid = pl.pallas_call(
        project_kernel,
        out_shape=[jax.ShapeDtypeStruct((part, model_width), jnp.bfloat16)] * n_out
        + [jax.ShapeDtypeStruct((tok_count, model_width), jnp.float32)],
        in_specs=in_vmem(4) + [pl.BlockSpec(memory_space=pltpu.HBM)] + in_vmem(2),
        out_specs=in_vmem(n_out + 1),
        scratch_shapes=[
            pltpu.VMEM((tok_count, model_width), jnp.bfloat16),
            pltpu.VMEM(out_proj.shape, jnp.bfloat16),
            pltpu.SemaphoreType.DMA((4,)),
        ],
        compiler_params=pltpu.CompilerParams(vmem_limit_bytes=58 << 20),
        cost_estimate=pl.CostEstimate(
            flops=3 * tok_count * model_width * model_width,
            bytes_accessed=2 * model_width * model_width,
            transcendentals=0,
        ),
        name="project",
    )(mixed, out_gate, stream, head_gain[None], out_proj, ffn_gain[None], placing)
    return outs, resid


CHUNKS = 2


def body(
    stream,
    query_proj,
    key_proj,
    value_proj,
    out_gate,
    beta_logit,
    log_decay,
    head_gain,
    out_proj,
    ffn_gain,
    routes,
    route_weight,
    expert_gate,
    expert_up,
    expert_down,
):
    n_sp, n_dp = lax.axis_size("sp"), lax.axis_size("dp")
    tok_count, model_width = stream.shape[1:]
    chips = n_dp // 2
    to_neighbour = []
    for x in range(chips):
        to_neighbour.append((2 * ((x + 1) % chips), 2 * x))
        to_neighbour.append((2 * ((x - 1) % chips) + 1, 2 * x + 1))
    to_core = [(i, i ^ 1) for i in range(n_dp)]
    to_partner = [(i, (i + n_dp // 2) % n_dp) for i in range(n_dp)]

    def over_sp(tensor):
        return lax.all_to_all(tensor, "sp", split_axis=0, concat_axis=0, tiled=True)

    own = (expert_gate[0], expert_up[0], expert_down[0])
    near = tuple(lax.ppermute(w, "dp", to_core) for w in own)
    far = tuple(lax.ppermute(w, "dp", to_neighbour) for w in own)
    received = over_sp(packed_heads(query_proj, key_proj, value_proj, beta_logit))
    mixed = mixer(received, log_decay.reshape(-1, TOK))
    top_count = routes.shape[2]
    capacity = tok_count * top_count * 2 // n_sp
    piece = capacity // CHUNKS
    flat_routes = routes.reshape(-1)
    expert_ids = lax.broadcasted_iota(jnp.int32, (1, n_sp), 1)
    chosen = (flat_routes[:, None] == expert_ids).astype(jnp.int32)
    earlier = jnp.cumsum(chosen, axis=0) - chosen
    place = jnp.sum(earlier * chosen, axis=1)
    slot_ids = (place // piece) * (n_sp * piece) + flat_routes * piece + place % piece
    slot_grid = lax.broadcasted_iota(jnp.int32, (n_sp * capacity, 1, 1), 0)
    here = slot_grid == slot_ids.reshape(1, tok_count, top_count)
    placing = jnp.sum(here.astype(jnp.int32), axis=2).astype(jnp.bfloat16)
    share = jnp.sum(jnp.where(here, route_weight, 0.0), axis=2).T
    share_high, share_low = halves(share)
    outgoing, resid = project(
        over_sp(mixed), out_gate, stream, head_gain, out_proj, ffn_gain, placing, CHUNKS
    )

    *far, outgoing[-1] = lax.optimization_barrier((*far, outgoing[-1]))
    last = tuple(lax.ppermute(w, "dp", to_core) for w in far)
    mine, theirs = [], []
    for c in range(CHUNKS):
        arrived = over_sp(outgoing[c].reshape(n_sp, piece, model_width))
        mine.append(arrived.reshape(-1, model_width))
        theirs.append(lax.ppermute(arrived, "dp", to_partner).reshape(-1, model_width))
    weights = (own, near, tuple(far), last)
    turns = [("mine", 0)] + [("theirs", c) for c in range(CHUNKS)]
    turns += [("mine", c) for c in range(1, CHUNKS)]
    made, before = {}, ()
    for side, c in turns:
        rows = mine[c] if side == "mine" else theirs[c]
        before = tuple(expert_part([rows], weights, before))
        made[side, c] = before[0]
    result = resid
    for c in range(CHUNKS):
        back = lax.ppermute(made["theirs", c], "dp", to_partner)
        whole = (made["mine", c].astype(jnp.float32) + back.astype(jnp.float32)).astype(jnp.bfloat16)
        home = over_sp(whole.reshape(n_sp, piece, model_width)).reshape(-1, model_width)
        span = slice(c * n_sp * piece, (c + 1) * n_sp * piece)
        result = result + mm(share_high[:, span], home) + mm(share_low[:, span], home)
    return result.astype(jnp.bfloat16)[None]


def solution(mesh):
    return jax.shard_map(
        body,
        mesh=mesh,
        in_specs=(
            P("dp", "sp", None),
            P("dp", "sp", None),
            P("dp", "sp", None),
            P("dp", "sp", None),
            P("dp", "sp", None),
            P("dp", "sp", None),
            P("dp", "sp", None),
            P(),
            P(),
            P(),
            P("dp", "sp", None),
            P("dp", "sp", None),
            P("sp", None, "dp"),
            P("sp", None, "dp"),
            P("sp", "dp", None),
        ),
        out_specs=P("dp", "sp", None),
        check_vma=False,
    )
```

```python
import jax
import jax.numpy as jnp
from jax import lax
from jax.experimental import pallas as pl
from jax.experimental.pallas import tpu as pltpu
from jax.sharding import PartitionSpec as P


EPSILON = 1e-6
HEAD_DIM = 128
TOK = 128
BASE = 16
UNROLL = 8


def mm(a, b):
    return jnp.dot(a, b, preferred_element_type=jnp.float32)


def halves(a):
    high = a.astype(jnp.bfloat16)
    return high, (a - high.astype(jnp.float32)).astype(jnp.bfloat16)


def mm3(a, b):
    ah, al = halves(a)
    bh, bl = halves(b)
    return mm(ah, bh) + (mm(ah, bl) + mm(al, bh))


def unit_lower_inverses(lows, apart, cols):
    n = cols.shape[0]
    group = cols[:BASE] >> 4
    packs, invs = [], []
    for low in lows:
        packed = jnp.where(group == 0, low[:BASE], 0.0)
        for b in range(1, n // BASE):
            packed = packed + jnp.where(group == b, low[b * BASE : (b + 1) * BASE], 0.0)
        packs.append(packed)
        invs.append(jnp.where(apart[:BASE] & (BASE - 1) == 0, 1.0, 0.0))
    for j in range(BASE - 1):
        columns = [jnp.take_along_axis(packed, (group << 4) + j, axis=1) for packed in packs]
        invs = [inv - column * inv[j : j + 1] for inv, column in zip(invs, columns)]
    fulls = [
        jnp.concatenate([jnp.where(group == b, inv, 0.0) for b in range(n // BASE)], axis=0)
        for inv in invs
    ]
    for shift in range(4, n.bit_length() - 1):
        cross = apart >> shift == 1
        firsts = [mm3(jnp.where(cross, low, 0.0), full) for low, full in zip(lows, fulls)]
        seconds = [mm3(full, first) for full, first in zip(fulls, firsts)]
        fulls = [full - second for full, second in zip(fulls, seconds)]
    return fulls


def mixer_kernel(recv_ref, rate_ref, out_ref, vec_ref, step_ref, lhs_ref, add_ref, acc_ref):
    n_blk = recv_ref.shape[0]
    rows = lax.broadcasted_iota(jnp.int32, (TOK, TOK), 0)
    cols = lax.broadcasted_iota(jnp.int32, (TOK, TOK), 1)
    rate = rate_ref[...]
    before = jnp.where(rows <= cols, 1.0, 0.0)
    after = jnp.where(rows >= cols, 1.0, 0.0)
    fwd_sum = jnp.dot(rate, before, precision=lax.Precision.HIGHEST, preferred_element_type=jnp.float32)
    bwd_sum = jnp.dot(rate, after, precision=lax.Precision.HIGHEST, preferred_element_type=jnp.float32)
    for n in range(n_blk):
        logit = recv_ref[n, 3 * TOK : 3 * TOK + 16, :].astype(jnp.float32)[0:1]
        vec_ref[n, 0:1, :] = fwd_sum[n : n + 1]
        vec_ref[n, 1:2, :] = bwd_sum[n : n + 1]
        vec_ref[n, 2:3, :] = jax.nn.sigmoid(logit)
        vec_ref[n, 3:4, :] = jnp.broadcast_to(fwd_sum[n : n + 1, TOK - 1 : TOK], (1, TOK))
        vec_ref[n, 4:8, :] = jnp.zeros((4, TOK), jnp.float32)

    def prepare(blocks):
        made, lows = [], []
        for n in blocks:
            query = recv_ref[n, 0:TOK, :]
            key = recv_ref[n, TOK : 2 * TOK, :]
            query_f = query.astype(jnp.float32)
            key_f = key.astype(jnp.float32)
            key_tf = key_f.T
            key_t = key_tf.astype(jnp.bfloat16)
            key_c = lax.rsqrt(jnp.sum(key_f * key_f, axis=1, keepdims=True) + EPSILON)
            key_r = lax.rsqrt(jnp.sum(key_tf * key_tf, axis=0, keepdims=True) + EPSILON)
            query_c = lax.rsqrt(jnp.sum(query_f * query_f, axis=1, keepdims=True) + EPSILON)
            query_c = query_c * HEAD_DIM ** (-0.5)
            vec_r = vec_ref[n]
            vec_c = vec_r.T
            kk = mm(key, key_t) * key_c * key_r
            qk = mm(query, key_t) * query_c * key_r
            for d in range(2):
                sum_r, sum_c = vec_r[d : d + 1], vec_c[:, d : d + 1]
                gap = sum_c - sum_r
                if d == 0:
                    decay = jnp.exp(jnp.where(rows >= cols, gap, -jnp.inf))
                    lows.append(jnp.where(rows > cols, kk * decay, 0.0) * vec_c[:, 2:3])
                else:
                    decay = jnp.exp(jnp.where(rows <= cols, gap, -jnp.inf))
                    turned = jnp.exp(jnp.where(rows >= cols, -gap, -jnp.inf))
                    lows.append(jnp.where(rows > cols, kk * turned, 0.0) * vec_r[2:3])
                lhs_ref[d, n, 0:TOK, :] = (qk * decay).astype(jnp.bfloat16)
                tail = key_r * jnp.exp(vec_r[3:4] - sum_r)
                lhs_ref[d, n, TOK:, :] = (key_tf * tail).astype(jnp.bfloat16)
            made.append((key_c, query_c, vec_c))
        solves = unit_lower_inverses(lows, rows ^ cols, cols)
        boths = []
        for i, n in enumerate(blocks):
            key_c, query_c, vec_c = made[i]
            beta_c = vec_c[:, 2:3]
            key_f = recv_ref[n, TOK : 2 * TOK, :].astype(jnp.float32)
            write = recv_ref[n, 2 * TOK : 3 * TOK, :].astype(jnp.float32) * beta_c
            for d in range(2):
                solve = solves[2 * i + d] if d == 0 else solves[2 * i + d].T
                grown = jnp.exp(vec_c[:, d : d + 1])
                rhs = jnp.concatenate([write, key_f * (beta_c * key_c * grown)], axis=1)
                boths.append(mm(solve.astype(jnp.bfloat16), rhs.astype(jnp.bfloat16)).astype(jnp.bfloat16))
        dones = [mm(lhs_ref[j % 2, blocks[j // 2]], both) for j, both in enumerate(boths)]
        for i, n in enumerate(blocks):
            key_c, query_c, vec_c = made[i]
            query_f = recv_ref[n, 0:TOK, :].astype(jnp.float32)
            for d in range(2):
                done = dones[2 * i + d]
                grown = query_c * jnp.exp(vec_c[:, d : d + 1])
                step_ref[d, n, 0:TOK, :] = (query_f * grown - done[:TOK, HEAD_DIM:]).astype(jnp.bfloat16)
                step_ref[d, n, TOK:, :] = done[TOK:, HEAD_DIM:].astype(jnp.bfloat16)
                add_ref[d, n] = done[TOK:, :HEAD_DIM]
            acc_ref[n] = dones[2 * i][:TOK, :HEAD_DIM] + dones[2 * i + 1][:TOK, :HEAD_DIM]

    def prepare_group(i, carry):
        prepare([i * UNROLL + u for u in range(UNROLL)])
        return carry

    lax.fori_loop(0, n_blk // UNROLL, prepare_group, 0)

    def walk(t, states):
        after_step = []
        for d, state in enumerate(states):
            n = t if d == 0 else n_blk - 1 - t
            high, low = halves(state)
            got = mm(step_ref[d, n], jnp.concatenate([high, low], axis=1))
            got = got[:, :HEAD_DIM] + got[:, HEAD_DIM:]
            acc_ref[n] = acc_ref[n] + got[:TOK]
            keep = jnp.exp(vec_ref[n][3:4])
            after_step.append(state * keep - got[TOK:] + add_ref[d, n])
        return tuple(after_step)

    zero = jnp.zeros((HEAD_DIM, HEAD_DIM), jnp.float32)
    lax.fori_loop(0, n_blk, walk, (zero, zero))
    out_ref[...] = acc_ref[...].astype(jnp.bfloat16)


def in_vmem(count):
    return [pl.BlockSpec(memory_space=pltpu.VMEM)] * count


def mixer(recv, rate):
    n_blk = recv.shape[0]
    return pl.pallas_call(
        mixer_kernel,
        out_shape=jax.ShapeDtypeStruct((n_blk, TOK, HEAD_DIM), jnp.bfloat16),
        in_specs=in_vmem(2),
        out_specs=in_vmem(1)[0],
        scratch_shapes=[
            pltpu.VMEM((n_blk, 8, TOK), jnp.float32),
            pltpu.VMEM((2, n_blk, 2 * TOK, HEAD_DIM), jnp.bfloat16),
            pltpu.VMEM((2, n_blk, 2 * TOK, HEAD_DIM), jnp.bfloat16),
            pltpu.VMEM((2, n_blk, HEAD_DIM, HEAD_DIM), jnp.float32),
            pltpu.VMEM((n_blk, TOK, HEAD_DIM), jnp.float32),
        ],
        compiler_params=pltpu.CompilerParams(vmem_limit_bytes=24 << 20),
        cost_estimate=pl.CostEstimate(flops=20 * 10**9, bytes_accessed=3 << 20, transcendentals=0),
        name="mixer",
    )(recv, rate)


def pack_kernel(query_ref, key_ref, value_ref, logit_ref, out_ref):
    logits = logit_ref[0].astype(jnp.float32).T.astype(jnp.bfloat16)
    for h in range(out_ref.shape[0]):
        lanes = slice(h * HEAD_DIM, (h + 1) * HEAD_DIM)
        out_ref[h, 0:TOK, :] = query_ref[0, :, lanes]
        out_ref[h, TOK : 2 * TOK, :] = key_ref[0, :, lanes]
        out_ref[h, 2 * TOK : 3 * TOK, :] = value_ref[0, :, lanes]
        out_ref[h, 3 * TOK :, :] = jnp.broadcast_to(logits[h : h + 1], (16, TOK))


def packed_heads(query_proj, key_proj, value_proj, beta_logit):
    n_heads = beta_logit.shape[2]
    return pl.pallas_call(
        pack_kernel,
        out_shape=jax.ShapeDtypeStruct((n_heads, 3 * TOK + 16, HEAD_DIM), jnp.bfloat16),
        in_specs=in_vmem(4),
        out_specs=in_vmem(1)[0],
        compiler_params=pltpu.CompilerParams(vmem_limit_bytes=16 << 20),
        cost_estimate=pl.CostEstimate(flops=10**6, bytes_accessed=3 << 20, transcendentals=0),
        name="pack",
    )(query_proj, key_proj, value_proj, beta_logit)


def expert_kernel(rows, *refs, n_parts, n_after, n_out):
    weights, refs = refs[: 3 * n_parts], refs[3 * n_parts + n_after :]
    outs, bufs, acc, sems = refs[:n_out], refs[n_out : n_out + 3], refs[n_out + 3], refs[n_out + 4]
    for s in range(n_parts):
        for k in range(3):
            pltpu.make_async_copy(weights[3 * s + k], bufs[k].at[s], sems.at[k, s]).start()
    acc[...] = jnp.zeros(acc.shape, jnp.float32)

    def part(s, carry):
        for k in range(3):
            pltpu.make_async_copy(weights[k], bufs[k].at[s], sems.at[k, s]).wait()
        gate_act = mm(rows[...], bufs[0][s])
        up_act = mm(rows[...], bufs[1][s])
        hidden = (jax.nn.silu(gate_act) * up_act).astype(jnp.bfloat16)
        acc[...] += mm(hidden, bufs[2][s])
        return carry

    lax.fori_loop(0, n_parts, part, 0)
    peers = outs[0].shape[0]
    whole = acc[...].reshape(peers, acc.shape[0] // peers, acc.shape[1])
    at = 0
    for out in outs:
        out[...] = whole[:, at : at + out.shape[1]].astype(jnp.bfloat16)
        at += out.shape[1]


def expert_part(rows, weights, peers, pieces, after=()):
    n_parts = len(weights)
    count, width = rows.shape
    units = weights[0][0].shape[1]
    flat = [w for part in weights for w in part]
    return pl.pallas_call(
        lambda *refs: expert_kernel(
            *refs, n_parts=n_parts, n_after=len(after), n_out=len(pieces)
        ),
        out_shape=[jax.ShapeDtypeStruct((peers, p, width), jnp.bfloat16) for p in pieces],
        in_specs=in_vmem(1) + [pl.BlockSpec(memory_space=pltpu.HBM)] * (len(flat) + len(after)),
        out_specs=in_vmem(len(pieces)),
        scratch_shapes=[pltpu.VMEM((n_parts, *w.shape), jnp.bfloat16) for w in weights[0]]
        + [pltpu.VMEM(rows.shape, jnp.float32)]
        + [pltpu.SemaphoreType.DMA((3, n_parts))],
        compiler_params=pltpu.CompilerParams(vmem_limit_bytes=52 << 20),
        cost_estimate=pl.CostEstimate(
            flops=6 * count * width * units * n_parts,
            bytes_accessed=6 * width * units * n_parts,
            transcendentals=0,
        ),
    )(rows, *flat, *after)


def project_kernel(
    mixed_ref, gate_ref, stream_ref, head_gain_ref, proj_hbm, ffn_gain_ref, placing_ref, *refs
):
    *outs, resid_ref, gated_ref, proj_ref, sems = refs
    parts = sems.shape[0]
    deep = proj_ref.shape[0] // parts
    copies = []
    for k in range(parts):
        span = slice(k * deep, (k + 1) * deep)
        copies.append(
            pltpu.make_async_copy(proj_hbm.at[span, :], proj_ref.at[span, :], sems.at[k])
        )
        copies[-1].start()
    for h in range(mixed_ref.shape[0]):
        lanes = slice(h * HEAD_DIM, (h + 1) * HEAD_DIM)
        head = mixed_ref[h].astype(jnp.float32)
        scale = lax.rsqrt(jnp.mean(head * head, axis=1, keepdims=True) + EPSILON)
        gate = jax.nn.silu(gate_ref[0, :, lanes].astype(jnp.float32))
        gated_ref[:, lanes] = (head * scale * head_gain_ref[...] * gate).astype(jnp.bfloat16)
    resid = stream_ref[0].astype(jnp.float32)
    for k in range(parts):
        span = slice(k * deep, (k + 1) * deep)
        copies[k].wait()
        resid = resid + mm(gated_ref[:, span], proj_ref[span, :])
    resid_ref[...] = resid
    scale = lax.rsqrt(jnp.mean(resid * resid, axis=1, keepdims=True) + EPSILON)
    ffn_in = (resid * scale * ffn_gain_ref[...]).astype(jnp.bfloat16)
    at = 0
    for out in outs:
        out[...] = mm(placing_ref[at : at + out.shape[0], :], ffn_in).astype(jnp.bfloat16)
        at += out.shape[0]


def project(mixed, out_gate, stream, head_gain, out_proj, ffn_gain, placing, n_out):
    tok_count, model_width = stream.shape[1:]
    part = placing.shape[0] // n_out
    *outs, resid = pl.pallas_call(
        project_kernel,
        out_shape=[jax.ShapeDtypeStruct((part, model_width), jnp.bfloat16)] * n_out
        + [jax.ShapeDtypeStruct((tok_count, model_width), jnp.float32)],
        in_specs=in_vmem(4) + [pl.BlockSpec(memory_space=pltpu.HBM)] + in_vmem(2),
        out_specs=in_vmem(n_out + 1),
        scratch_shapes=[
            pltpu.VMEM((tok_count, model_width), jnp.bfloat16),
            pltpu.VMEM(out_proj.shape, jnp.bfloat16),
            pltpu.SemaphoreType.DMA((4,)),
        ],
        compiler_params=pltpu.CompilerParams(vmem_limit_bytes=58 << 20),
        cost_estimate=pl.CostEstimate(
            flops=3 * tok_count * model_width * model_width,
            bytes_accessed=2 * model_width * model_width,
            transcendentals=0,
        ),
        name="project",
    )(mixed, out_gate, stream, head_gain[None], out_proj, ffn_gain[None], placing)
    return outs, resid


CHUNKS = 2


def body(
    stream,
    query_proj,
    key_proj,
    value_proj,
    out_gate,
    beta_logit,
    log_decay,
    head_gain,
    out_proj,
    ffn_gain,
    routes,
    route_weight,
    expert_gate,
    expert_up,
    expert_down,
):
    n_sp, n_dp = lax.axis_size("sp"), lax.axis_size("dp")
    tok_count, model_width = stream.shape[1:]
    chips = n_dp // 2
    to_neighbour = []
    for x in range(chips):
        to_neighbour.append((2 * ((x + 1) % chips), 2 * x))
        to_neighbour.append((2 * ((x - 1) % chips) + 1, 2 * x + 1))
    to_core = [(i, i ^ 1) for i in range(n_dp)]
    to_partner = [(i, (i + n_dp // 2) % n_dp) for i in range(n_dp)]

    def over_sp(tensor):
        return lax.all_to_all(tensor, "sp", split_axis=0, concat_axis=0, tiled=True)

    own = (expert_gate[0], expert_up[0], expert_down[0])
    near = tuple(lax.ppermute(w, "dp", to_core) for w in own)
    far = tuple(lax.ppermute(w, "dp", to_neighbour) for w in own)
    received = over_sp(packed_heads(query_proj, key_proj, value_proj, beta_logit))
    mixed = mixer(received, log_decay.reshape(-1, TOK))
    top_count = routes.shape[2]
    capacity = tok_count * top_count * 2 // n_sp
    piece = capacity // CHUNKS
    flat_routes = routes.reshape(-1)
    expert_ids = lax.broadcasted_iota(jnp.int32, (1, n_sp), 1)
    chosen = (flat_routes[:, None] == expert_ids).astype(jnp.int32)
    earlier = jnp.cumsum(chosen, axis=0) - chosen
    place = jnp.sum(earlier * chosen, axis=1)
    slot_ids = (place // piece) * (n_sp * piece) + flat_routes * piece + place % piece
    slot_grid = lax.broadcasted_iota(jnp.int32, (n_sp * capacity, 1, 1), 0)
    here = slot_grid == slot_ids.reshape(1, tok_count, top_count)
    placing = jnp.sum(here.astype(jnp.int32), axis=2).astype(jnp.bfloat16)
    half = piece // 2
    late = (place % piece) // half
    home_ids = (CHUNKS - 1 + late) * (n_sp * half) + flat_routes * half + place % half
    home_ids = (CHUNKS - 1) * (n_sp * half) + home_ids
    home_ids = jnp.where(place // piece < CHUNKS - 1, slot_ids, home_ids)
    there = slot_grid == home_ids.reshape(1, tok_count, top_count)
    share = jnp.sum(jnp.where(there, route_weight, 0.0), axis=2).T
    share_high, share_low = halves(share)
    outgoing, resid = project(
        over_sp(mixed), out_gate, stream, head_gain, out_proj, ffn_gain, placing, CHUNKS
    )

    *far, outgoing[-1] = lax.optimization_barrier((*far, outgoing[-1]))
    last = tuple(lax.ppermute(w, "dp", to_core) for w in far)
    mine, theirs = [], []
    for c in range(CHUNKS):
        arrived = over_sp(outgoing[c].reshape(n_sp, piece, model_width))
        mine.append(arrived.reshape(-1, model_width))
        theirs.append(lax.ppermute(arrived, "dp", to_partner).reshape(-1, model_width))
    weights = (own, near, tuple(far), last)
    pieces = [[piece]] * (CHUNKS - 1) + [[half, half]]
    turns = [(side, c) for c in range(CHUNKS) for side in ("mine", "theirs")]
    made, before = {}, ()
    for side, c in turns:
        rows = mine[c] if side == "mine" else theirs[c]
        made[side, c] = expert_part(rows, weights, n_sp, pieces[c], before)
        before = (made[side, c][0],)
    kept = [out for c in range(CHUNKS) for out in made["mine", c]]
    lent = [out for c in range(CHUNKS) for out in made["theirs", c]]
    result, at = resid, 0
    for c in range(len(kept)):
        back = lax.ppermute(lent[c], "dp", to_partner)
        whole = kept[c].astype(jnp.float32) + back.astype(jnp.float32)
        whole = whole.astype(jnp.bfloat16)
        home = over_sp(whole).reshape(-1, model_width)
        span = slice(at, at + home.shape[0])
        result = result + mm(share_high[:, span], home) + mm(share_low[:, span], home)
        at += home.shape[0]
    return result.astype(jnp.bfloat16)[None]


def solution(mesh):
    return jax.shard_map(
        body,
        mesh=mesh,
        in_specs=(
            P("dp", "sp", None),
            P("dp", "sp", None),
            P("dp", "sp", None),
            P("dp", "sp", None),
            P("dp", "sp", None),
            P("dp", "sp", None),
            P("dp", "sp", None),
            P(),
            P(),
            P(),
            P("dp", "sp", None),
            P("dp", "sp", None),
            P("sp", None, "dp"),
            P("sp", None, "dp"),
            P("sp", "dp", None),
        ),
        out_specs=P("dp", "sp", None),
        check_vma=False,
    )
```
